256 devices in a mesh: kv: 32 (over z, x), tp: 8 (over y, core).
Axes of the slice: x: 4, y: 4, z: 8, core: 2. Of those that a mesh axis runs over, the one named last changes fastest.
Arguments:
- queries: bfloat16 [4096, 2048], P('kv', 'tp'), may hold values from -6 to 6
- keys: bfloat16 [4096, 2048], P('kv', 'tp'), may hold values from -6 to 6
- values: bfloat16 [4096, 2048], P('kv', 'tp'), may hold values from -6 to 6
- attended: bfloat16 [4096, 2048], P('kv', 'tp'), may hold values from -6 to 6
- cotangent: bfloat16 [4096, 2048], P('kv', 'tp'), may hold values from -96 to 96
- log_totals: float32 [32, 4096], P('tp', 'kv'), may hold values from 4 to 7
- block_picks: int32 [32, 64, 8], P('tp', 'kv'), may hold values from -1 to 62, as said below
- normed: bfloat16 [4096, 4096], P('kv', 'tp'), may hold values from -6 to 6
Outputs:
- grad_queries: bfloat16 [4096, 2048], P('kv', 'tp')
- grad_keys: bfloat16 [4096, 2048], P('kv', 'tp')
- grad_values: bfloat16 [4096, 2048], P('kv', 'tp')
- grad_weight: float32 [4096, 2048], P('kv', 'tp')
The draws below stay inside these ranges and needn't reach their ends.
Inputs may be any that keep to these rules, and one draw needn't show every extreme that they name: `block_picks`: row c of head h names at most 8 distinct blocks below c, followed by -1 in the other slots. One key block is named by at most 16 query blocks of one head, and in every draw each head has a block named exactly 16 times.
All inputs are finite; a program needn't handle non-finite values.
Results may differ from the reference program's by a relative error of at most 0.0069.
Values may be sent and summed in bfloat16 or wider, within the bound.
A program may use at most 128 MiB of HBM per device.

```python
import jax
import jax.numpy as jnp
from jax import lax

D = 4096
H = 32
DH = 64
BLOCK = 64
SEL = 8
TOKENS = 4096
NQB = 64
MOST = 16


def draw_block_picks(key, part):
    key_jitter, key_hot = jax.random.split(jax.random.fold_in(key, 17))
    jitter = jax.random.randint(key_jitter, (H, NQB, NQB), 0, 2 ** 24 // NQB)
    hot_ids = jax.random.randint(key_hot, (H, 3), 0, max(1, NQB // 4))
    block_ids = jnp.arange(NQB)

    def one_head(jitter_h, hot_h):
        others = jnp.any(block_ids[:, None] == hot_h[None, 1:], axis=1)

        def advance(tallies, qblock):
            levels = jnp.where(others, 2, 1)
            levels = jnp.where(block_ids == qblock - NQB // 2, 3, levels)
            levels = jnp.where(block_ids == qblock - 1, 4, levels)
            levels = jnp.where(block_ids == hot_h[0], 5, levels)
            usable = (block_ids < qblock) & (tallies < MOST)
            scores = jnp.where(usable, levels * 2 ** 24 + jitter_h[qblock] * NQB + block_ids, -(block_ids + 1))
            top_vals, chosen_ids = lax.top_k(scores, SEL)
            row_ids = jnp.where(top_vals >= 0, chosen_ids, -1).astype(jnp.int32)
            tallies = tallies + jnp.sum((row_ids[:, None] == block_ids[None, :]).astype(jnp.int32), axis=0)
            return (tallies, row_ids)
        _, table = lax.scan(advance, jnp.zeros((NQB,), jnp.int32), jnp.arange(NQB))
        return table
    return jax.vmap(one_head)(jitter, hot_ids).astype(jnp.int32)


def spiked(entries, key, source, target, parts, factor):
    def block_of(dim):
        return (jnp.arange(entries.shape[dim]) // (entries.shape[dim] // parts)).reshape((-1,) + (1,) * (entries.ndim - 1 - dim))

    one_side = jax.random.permutation(key, parts)[block_of(target)]
    other_side = (block_of(target) + parts // 2) % parts
    return jnp.where((block_of(source) == one_side) | (block_of(source) == other_side), factor * entries, entries)


def block_levels(rng, shape, cuts, smallest, high):
    def one(position, blocks):
        steps = jax.random.uniform(jax.random.fold_in(jax.random.fold_in(rng, 6), position), (blocks,), jnp.float32, smallest / len(cuts), high / len(cuts))
        return jnp.repeat(jnp.exp(steps), shape[position] // blocks).reshape((-1,) + (1,) * (len(shape) - position - 1))

    loudness = one(*cuts[0])
    for cut in cuts[1:]:
        loudness = loudness * one(*cut)
    return loudness


def centred(stream_key, shape, width, most, shards=(), held_as=jnp.bfloat16):
    values = width * jax.random.normal(stream_key, shape, jnp.float32)
    if shards:
        values = values * block_levels(stream_key, shape, shards, -0.22, 0.18)
    return jnp.clip(values, -most, most).astype(held_as)


def heavy_noise(rng, extent, scale, limit, cuts, heavy, kind=jnp.bfloat16):
    result = scale * jax.random.normal(rng, extent, jnp.float32)
    if cuts:
        result = result * block_levels(rng, extent, cuts, -0.22, 0.18)
    return jnp.clip(spiked(result, jax.random.fold_in(rng, 3), *heavy), -limit, limit).astype(kind)


def setup_inputs(seed: int = 0) -> dict:
    splits = jax.random.split(jax.random.key(seed), 9)
    queries = centred(splits[0], (TOKENS, H * DH), 1.0, 6.0, ((0, 32), (1, 8)))
    keys = centred(splits[1], (TOKENS, H * DH), 1.0, 6.0, ((0, 32), (1, 8)))
    values = centred(splits[2], (TOKENS, H * DH), 1.0, 6.0, ((0, 32), (1, 8)))
    attended = centred(splits[3], (TOKENS, H * DH), 1.0, 6.0, ((0, 32), (1, 8)))
    cotangent = centred(splits[4], (TOKENS, H * DH), 16.0, 96.0, ((0, 32), (1, 8)))
    log_totals = jnp.clip(4.0 + 3.0 * jax.random.uniform(splits[5], (H, TOKENS), jnp.float32) ** block_levels(splits[5], (H, TOKENS), ((0, 8), (1, 32)), -0.2, 0.2), 4.0, 7.0)
    block_picks = draw_block_picks(jax.random.fold_in(splits[8], 71), 0)
    normed = heavy_noise(splits[7], (TOKENS, D), 1.0, 6.0, ((0, 32), (1, 8)), (0, 1, 32, 2.75))
    return {"queries": queries, "keys": keys, "values": values, "attended": attended, "cotangent": cotangent, "log_totals": log_totals, "block_picks": block_picks, "normed": normed}


def tile_grads(q_tile, k_tile, v_tile, g_tile, log_total, row_dots, allowed):
    scale = q_tile.shape[-1] ** -0.5
    scores = jnp.einsum('...qd,...kd->...qk', q_tile, k_tile) * scale
    probs = jnp.where(allowed, jnp.exp(scores - log_total[..., None]), 0.0)
    probs_low = lax.optimization_barrier(probs.astype(jnp.bfloat16)).astype(jnp.float32)
    grad_v = jnp.einsum('...qk,...qd->...kd', probs_low, g_tile)
    grad_p = jnp.einsum('...qd,...kd->...qk', g_tile, v_tile)
    grad_s = (probs * (grad_p - row_dots[..., None])).astype(jnp.bfloat16)
    grad_s = lax.optimization_barrier(grad_s).astype(jnp.float32)
    grad_q = jnp.einsum('...qk,...kd->...qd', grad_s, k_tile) * scale
    grad_k = jnp.einsum('...qk,...qd->...kd', grad_s, q_tile) * scale
    return grad_q, grad_k, grad_v


def by_head(matrix):
    return matrix.astype(jnp.float32).reshape(NQB, BLOCK, H, DH).transpose(2, 0, 1, 3)


def to_rows(tensor):
    return tensor.transpose(1, 2, 0, 3).reshape(NQB * BLOCK, H * DH)


def reference(queries, keys, values, attended, cotangent, log_totals, block_picks, normed):
    causal = jnp.tril(jnp.ones((BLOCK, BLOCK), bool))
    log_heads = log_totals.reshape(H, NQB, BLOCK)

    def per_head(operands):
        q_h, k_h, v_h, o_h, g_h, l_h, picked = operands
        row_dots = jnp.sum(g_h * o_h, axis=-1)
        dq_diag, dk_diag, dv_diag = tile_grads(q_h, k_h, v_h, g_h, l_h, row_dots, causal)
        present = picked >= 0
        clamped = jnp.maximum(picked, 0)
        k_sel = k_h[clamped]
        v_sel = v_h[clamped]
        tile_shape = k_sel.shape
        q_rep = jnp.broadcast_to(q_h[:, None], tile_shape)
        g_rep = jnp.broadcast_to(g_h[:, None], tile_shape)
        l_rep = jnp.broadcast_to(l_h[:, None], tile_shape[:3])
        d_rep = jnp.broadcast_to(row_dots[:, None], tile_shape[:3])
        allowed = jnp.broadcast_to(present[:, :, None, None], tile_shape[:3] + (BLOCK,))
        dq_sel, dk_sel, dv_sel = tile_grads(q_rep, k_sel, v_sel, g_rep, l_rep, d_rep, allowed)
        segments = jnp.where(present, picked, NQB).reshape(-1).astype(jnp.int32)
        dk_sum = jax.ops.segment_sum(dk_sel.reshape(-1, BLOCK, DH), segments, num_segments=NQB + 1)[:NQB]
        dv_sum = jax.ops.segment_sum(dv_sel.reshape(-1, BLOCK, DH), segments, num_segments=NQB + 1)[:NQB]
        return dq_diag + jnp.sum(dq_sel, axis=1), dk_diag + dk_sum, dv_diag + dv_sum

    grad_q, grad_k, grad_v = lax.map(per_head, (by_head(queries), by_head(keys), by_head(values),
                                                by_head(attended), by_head(cotangent), log_heads, block_picks))
    grad_queries = to_rows(grad_q).astype(jnp.bfloat16)
    grad_weight = jnp.dot(normed.T, grad_queries, preferred_element_type=jnp.float32)
    return grad_queries, to_rows(grad_k).astype(jnp.bfloat16), to_rows(grad_v).astype(jnp.bfloat16), grad_weight
```

```python
import functools
import math

import jax
import jax.numpy as jnp
from jax import lax
from jax.experimental import pallas as pl
from jax.experimental.pallas import tpu as pltpu
from jax.sharding import PartitionSpec as P

MESH = pl.DeviceIdType.MESH
BLOCK = 64
NZ, NX, NT = 8, 4, 8
ROWS = 128
WIDTH = 256
HEADS, DH = 4, 64
SEL = 8
FEATS = 128
KB = 2 * NX
NEVER = 1e30
F32, BF16 = jnp.float32, jnp.bfloat16

UP, DOWN = NZ // 2, NZ // 2 - 1


def up_slot(s):
    return 2 * s - 1


def down_slot(s):
    return 2 * s if s < NZ // 2 else NZ - 1


OFFSETS = [0] + [None] * (NZ - 1)
for _s in range(1, NZ // 2 + 1):
    OFFSETS[up_slot(_s)] = -_s
for _s in range(1, NZ // 2):
    OFFSETS[down_slot(_s)] = _s
PAIR = [0] + [OFFSETS.index(-o) if -o in OFFSETS else NZ - 1 for o in OFFSETS[1:]]


def nt_dot(a, b):
    return lax.dot_general(a, b, (((1,), (1,)), ((), ())), preferred_element_type=F32)


def nn_dot(a, b):
    return lax.dot_general(a, b, (((1,), (0,)), ((), ())), preferred_element_type=F32)


def diagonal_heads(m):
    lane_head = lax.broadcasted_iota(jnp.int32, (DH, WIDTH), 1) // DH
    out = m[(HEADS - 1) * DH :]
    for h in range(HEADS - 1):
        out = jnp.where(lane_head == h, m[h * DH : (h + 1) * DH], out)
    return out


def kernel(
    q_ref, k_ref, v_ref, o_ref, g_ref, l_ref, pick_ref, n_ref,
    gq_ref, gk_ref, gv_ref, gw_ref,
    qa, ga, lm, pk, kx, vx, kbd, vbd, kbt, ps, ds, dqs, dqr, dq0,
    nx, nt, ntt, dqx, dks, dvs, dkr, dvr, dk0, dv0, gws, gwr, gw0,
    send_sem, recv_sem,
):
    kv = lax.axis_index("kv")
    t = lax.axis_index("tp")
    a = kv // NX
    b = kv % NX
    scale = DH**-0.5
    log2e = 1.0 / math.log(2.0)

    def at_z(off):
        return {"kv": ((a + NZ + off) % NZ) * NX + b, "tp": t}

    def at_x(r):
        return {"kv": a * NX + (b + r) % NX, "tp": t}

    def at_t(r):
        return {"kv": kv, "tp": (t + r) % NT}

    started = []
    counts = [0]

    def sems(n):
        first = counts[0]
        counts[0] += n
        return first

    S_Q, S_L, S_P, S_G = sems(NZ), sems(NZ), sems(NZ), sems(NZ)
    S_K, S_V, S_N, S_T = sems(NX), sems(NX), sems(NX), sems(NT)
    S_DQ, S_DK, S_DV, S_X, S_W = sems(NZ), sems(NX), sems(NX), sems(NX), sems(NZ)

    def send(src, dst, at_mine, at_theirs, dev):
        copy = pltpu.make_async_remote_copy(
            src_ref=src, dst_ref=dst, send_sem=send_sem.at[at_mine], recv_sem=recv_sem.at[at_theirs],
            device_id=dev, device_id_type=MESH,
        )
        copy.start()
        started.append(copy)

    def arrived(dst, at_mine, dev):
        pltpu.make_async_remote_copy(
            src_ref=dst, dst_ref=dst, send_sem=send_sem.at[at_mine], recv_sem=recv_sem.at[at_mine],
            device_id=dev, device_id_type=MESH,
        ).wait_recv()

    def slot_rows(slot):
        return pl.ds(slot * ROWS, ROWS)

    barrier = pltpu.get_barrier_semaphore()
    for off in range(1, NZ):
        pl.semaphore_signal(barrier, inc=1, device_id=at_z(off), device_id_type=MESH)
    for r in range(1, NX):
        pl.semaphore_signal(barrier, inc=1, device_id=at_x(r), device_id_type=MESH)
    for r in range(1, NT):
        pl.semaphore_signal(barrier, inc=1, device_id=at_t(r), device_id_type=MESH)

    lane = lax.broadcasted_iota(jnp.int32, (8, ROWS), 1)
    sub = lax.broadcasted_iota(jnp.int32, (8, ROWS), 0)
    for h in range(HEADS):
        rows = jnp.zeros((8, ROWS), jnp.int32)
        for s in range(SEL):
            spread = jnp.where(lane < BLOCK, pick_ref[h, 0, s], pick_ref[h, 1, s])
            rows = jnp.where(sub == s, spread, rows)
        pk[0, h * 8 : (h + 1) * 8, :] = rows
    prod = g_ref[...].astype(F32) * o_ref[...].astype(F32)
    high = prod.astype(BF16)
    low = (prod - high.astype(F32)).astype(BF16)
    ones = (
        lax.broadcasted_iota(jnp.int32, (8, WIDTH), 1) // DH == lax.broadcasted_iota(jnp.int32, (8, WIDTH), 0)
    ).astype(BF16)
    dots = nt_dot(ones, high) + nt_dot(ones, low)
    lm[0, 0:HEADS, :] = l_ref[...] * log2e
    lm[0, HEADS : 2 * HEADS, :] = dots[0:HEADS]
    qa[slot_rows(0), :] = q_ref[...]
    ga[slot_rows(0), :] = g_ref[...]

    pl.semaphore_wait(barrier, (NZ - 1) + (NX - 1) + (NT - 1))

    def ring(s, down, first, ref, own, by_rows):
        slot_of = down_slot if down else up_slot
        there = slot_of(s + 1)
        dst = ref.at[slot_rows(there), :] if by_rows else ref.at[there]
        if s == 0:
            src = own
        else:
            src = ref.at[slot_rows(slot_of(s)), :] if by_rows else ref.at[slot_of(s)]
        send(src, dst, first + there, first + there, at_z(-1 if down else 1))

    def ring_arrived(s, down, first, ref, by_rows):
        slot = (down_slot if down else up_slot)(s)
        dst = ref.at[slot_rows(slot), :] if by_rows else ref.at[slot]
        arrived(dst, first + slot, at_z(1 if down else -1))

    streams = (
        (S_Q, qa, q_ref, True, UP, DOWN),
        (S_L, lm, lm.at[0], False, UP, DOWN),
        (S_P, pk, pk.at[0], False, UP, DOWN),
        (S_G, ga, g_ref, True, DOWN, UP),
    )

    def ring_step(s):
        for first, ref, own, by_rows, up, down in streams:
            for going_down, limit in ((False, up), (True, down)):
                if 0 < s <= limit:
                    ring_arrived(s, going_down, first, ref, by_rows)
                if s < limit:
                    ring(s, going_down, first, ref, own, by_rows)

    ring_step(0)
    for r in (1, 3, 2):
        send(k_ref, kx.at[NX - r], S_K + r, S_K + NX - r, at_x(r))
        send(v_ref, vx.at[NX - r], S_V + r, S_V + NX - r, at_x(r))
    for r in (1, 3, 2):
        there = (b + r) % NX
        cols = pl.ds(pl.multiple_of(there * FEATS, FEATS), FEATS)
        send(n_ref.at[:, cols], nx.at[NX - r], S_N + r, S_N + NX - r, at_x(r))
    nx[0] = n_ref[:, pl.ds(pl.multiple_of(b * FEATS, FEATS), FEATS)]

    lane_head = lax.broadcasted_iota(jnp.int32, (BLOCK, WIDTH), 1) // DH
    t_head = lax.broadcasted_iota(jnp.int32, (WIDTH, 2 * BLOCK), 0) // DH
    t_half = lax.broadcasted_iota(jnp.int32, (WIDTH, 2 * BLOCK), 1) // BLOCK

    def lay_out_keys(r, keys, vals):
        for i in range(2):
            j = 2 * r + i
            kb = keys[i * BLOCK : (i + 1) * BLOCK, :]
            vb = vals[i * BLOCK : (i + 1) * BLOCK, :]
            zero = jnp.zeros_like(kb)
            for h in range(HEADS):
                kbd[j, h * DH : (h + 1) * DH, :] = jnp.where(lane_head == h, kb, zero)
                vbd[j, h * DH : (h + 1) * DH, :] = jnp.where(lane_head == h, vb, zero)
            turned = jnp.concatenate([kb, kb], axis=0).T
            for hh in range(HEADS // 2):
                kbt[:, pl.ds(j * WIDTH + hh * ROWS, ROWS)] = jnp.where(
                    t_head == 2 * hh + t_half, turned, jnp.zeros_like(turned)
                )

    lay_out_keys(0, k_ref[...], v_ref[...])

    key_at = lax.broadcasted_iota(jnp.int32, (BLOCK, ROWS), 0)
    row_at = lax.broadcasted_iota(jnp.int32, (BLOCK, ROWS), 1)

    def tile(j, slot, count, own_block=None):
        wide = count * ROWS
        rows = pl.ds(slot * ROWS, wide)
        scores = nt_dot(kbd[j], qa[rows, :])
        gp = nt_dot(vbd[j], ga[rows, :])
        block_id = a * KB + 2 * ((b + j // 2) % NX) + j % 2
        for h in range(HEADS):
            offs = []
            for c in range(count):
                hit = jnp.where(pk[slot + c, h * 8 : (h + 1) * 8, :] == block_id, 1.0, 0.0)
                hit = jnp.max(hit, axis=0, keepdims=True)
                offs.append(jnp.where(hit > 0.5, lm[slot + c, h : h + 1, :], NEVER))
            off = offs[0] if count == 1 else jnp.concatenate(offs, axis=1)
            if own_block is not None:
                ok = key_at <= row_at % BLOCK
                own = jnp.where(ok, jnp.broadcast_to(lm[0, h : h + 1, :], ok.shape), NEVER)
                off = jnp.where(row_at // BLOCK == own_block, own, jnp.broadcast_to(off, ok.shape))
            dots_row = [lm[slot + c, HEADS + h : HEADS + h + 1, :] for c in range(count)]
            dots_row = dots_row[0] if count == 1 else jnp.concatenate(dots_row, axis=1)
            part = slice(h * DH, (h + 1) * DH)
            p = jnp.exp2(scores[part] * (scale * log2e) - off)
            ps[j, part, pl.ds(slot * ROWS, wide)] = p.astype(BF16)
            ds[pl.ds(j * WIDTH + h * DH, DH), pl.ds(slot * ROWS, wide)] = (p * (gp[part] - dots_row)).astype(BF16)

    def tiles(slot, count, first=0):
        def body(j, carry):
            tile(j, slot, count)
            return carry

        lax.fori_loop(first, KB, body, 0)

    def query_grads(slot, count):
        part = nn_dot(kbt[...], ds[:, pl.ds(slot * ROWS, count * ROWS)])
        for c in range(count):
            k = slot + c
            piece = part[:, c * ROWS : (c + 1) * ROWS]
            if k == 0:
                dq0[...] = piece
            else:
                dqs[k] = piece.astype(BF16)
        for c in range(count):
            k = slot + c
            if k:
                send(dqs.at[k], dqr.at[PAIR[k]], S_DQ + k, S_DQ + PAIR[k], at_z(OFFSETS[k]))

    ring_step(1)
    for r in (1, 3, 2):
        arrived(kx.at[r], S_K + r, at_x(r))
        arrived(vx.at[r], S_V + r, at_x(r))
        lay_out_keys(r, kx[r], vx[r])
    for r in (1, 3, 2):
        arrived(nx.at[r], S_N + r, at_x(r))
    ring_step(2)
    for r in range(1, NT):
        send(nx, nt.at[t], S_T + r, S_T + NT - r, at_t(r))
    nt[t] = nx[...]
    for i in range(2):
        tile(i, 0, 1, own_block=i)
    tiles(0, 1, 2)
    query_grads(0, 1)
    tiles(1, 2)
    query_grads(1, 2)
    ring_step(3)
    tiles(3, 2)
    query_grads(3, 2)
    tiles(5, 2)
    query_grads(5, 2)
    ring_step(4)
    tiles(7, 1)
    query_grads(7, 1)

    def key_grads(r):
        for i in range(2):
            j = 2 * r + i
            gv = diagonal_heads(nn_dot(ps[j], ga[...]))
            gk = diagonal_heads(nn_dot(ds[pl.ds(j * WIDTH, WIDTH), :], qa[...])) * scale
            part = slice(i * BLOCK, (i + 1) * BLOCK)
            if r == 0:
                dv0[part, :] = gv
                dk0[part, :] = gk
            else:
                dvs[r, part, :] = gv.astype(BF16)
                dks[r, part, :] = gk.astype(BF16)

    key_grads(1)
    key_grads(2)
    for r in range(1, NT):
        arrived(nt.at[(t + r) % NT], S_T + r, at_t(r))
    for z in range(NZ):
        for r in range(NX):
            ntt[z, :, r * ROWS : (r + 1) * ROWS] = nt[z, r].T

    total = dq0[...]
    for k in range(1, NZ):
        arrived(dqr.at[k], S_DQ + k, at_z(OFFSETS[k]))
    for k in range(1, NZ):
        total = total + dqr[k].astype(F32)
    grad_q = (total * scale).T.astype(BF16)
    dqx[0] = grad_q
    for r in (2, 1, 3):
        send(dqx.at[0], dqx.at[NX - r], S_X + r, S_X + NX - r, at_x(r))
    gq_ref[...] = grad_q
    for r in (1, 2):
        send(dks.at[r], dkr.at[NX - r], S_DK + r, S_DK + NX - r, at_x(r))
        send(dvs.at[r], dvr.at[NX - r], S_DV + r, S_DV + NX - r, at_x(r))
    key_grads(3)
    for r in (3,):
        send(dks.at[r], dkr.at[NX - r], S_DK + r, S_DK + NX - r, at_x(r))
        send(dvs.at[r], dvr.at[NX - r], S_DV + r, S_DV + NX - r, at_x(r))
    key_grads(0)

    for r in (1, 3, 2):
        arrived(dqx.at[r], S_X + r, at_x(r))
    dq_row = dqx[...].reshape(NX * ROWS, WIDTH)
    for k in (7, 5, 6, 3, 4, 1, 2, 0):
        piece = nn_dot(ntt[(a + NZ + OFFSETS[k]) % NZ], dq_row)
        if k == 0:
            gw0[...] = piece
        else:
            gws[k] = piece.astype(BF16)
            send(gws.at[k], gwr.at[PAIR[k]], S_W + k, S_W + PAIR[k], at_z(OFFSETS[k]))

    for r in (1, 3, 2):
        arrived(dkr.at[r], S_DK + r, at_x(r))
        arrived(dvr.at[r], S_DV + r, at_x(r))
    sum_k, sum_v = dk0[...], dv0[...]
    for r in range(1, NX):
        sum_k = sum_k + dkr[r].astype(F32)
        sum_v = sum_v + dvr[r].astype(F32)
    gk_ref[...] = sum_k.astype(BF16)
    gv_ref[...] = sum_v.astype(BF16)

    total_w = gw0[...]
    for k in range(1, NZ):
        arrived(gwr.at[k], S_W + k, at_z(OFFSETS[k]))
    for k in range(1, NZ):
        total_w = total_w + gwr[k].astype(F32)
    gw_ref[...] = total_w
    for copy in started:
        copy.wait_send()


def local(queries, keys, values, attended, cotangent, log_totals, block_picks, normed):
    vmem = pl.BlockSpec(memory_space=pltpu.VMEM)
    sem_count = 4 * NZ + 3 * NX + NT + NZ + 3 * NX + NZ
    b16 = lambda *shape: pltpu.VMEM(shape, BF16)
    f32 = lambda *shape: pltpu.VMEM(shape, F32)
    return pl.pallas_call(
        kernel,
        out_shape=(
            jax.ShapeDtypeStruct((ROWS, WIDTH), BF16),
            jax.ShapeDtypeStruct((ROWS, WIDTH), BF16),
            jax.ShapeDtypeStruct((ROWS, WIDTH), BF16),
            jax.ShapeDtypeStruct((FEATS, WIDTH), F32),
        ),
        in_specs=[vmem] * 6 + [pl.BlockSpec(memory_space=pltpu.SMEM), vmem],
        out_specs=(vmem,) * 4,
        scratch_shapes=[
            b16(NZ * ROWS, WIDTH), b16(NZ * ROWS, WIDTH), f32(NZ, 2 * HEADS, ROWS),
            pltpu.VMEM((NZ, HEADS * SEL, ROWS), jnp.int32),
            b16(NX, ROWS, WIDTH), b16(NX, ROWS, WIDTH),
            b16(KB, WIDTH, WIDTH), b16(KB, WIDTH, WIDTH), b16(WIDTH, KB * WIDTH),
            b16(KB, WIDTH, NZ * ROWS), b16(KB * WIDTH, NZ * ROWS),
            b16(NZ, WIDTH, ROWS), b16(NZ, WIDTH, ROWS), f32(WIDTH, ROWS),
            b16(NX, ROWS, FEATS), b16(NT, NX, ROWS, FEATS), b16(NZ, FEATS, NX * ROWS),
            b16(NX, ROWS, WIDTH),
            b16(NX, ROWS, WIDTH), b16(NX, ROWS, WIDTH), b16(NX, ROWS, WIDTH), b16(NX, ROWS, WIDTH),
            f32(ROWS, WIDTH), f32(ROWS, WIDTH),
            b16(NZ, FEATS, WIDTH), b16(NZ, FEATS, WIDTH), f32(FEATS, WIDTH),
            pltpu.SemaphoreType.DMA((sem_count,)),
            pltpu.SemaphoreType.DMA((sem_count,)),
        ],
        compiler_params=pltpu.CompilerParams(
            collective_id=0, has_side_effects=True, vmem_limit_bytes=48 * 1024 * 1024
        ),
        name="attention_grads",
    )(queries, keys, values, attended, cotangent, log_totals, block_picks, normed)


def solution(mesh):
    in_specs = (
        P("kv", "tp"),
        P("kv", "tp"),
        P("kv", "tp"),
        P("kv", "tp"),
        P("kv", "tp"),
        P("tp", "kv"),
        P("tp", "kv", None),
        P("kv", "tp"),
    )
    out_specs = (P("kv", "tp"), P("kv", "tp"), P("kv", "tp"), P("kv", "tp"))
    return jax.shard_map(local, mesh=mesh, in_specs=in_specs, out_specs=out_specs, check_vma=False)
```

```python
import functools
import math

import jax
import jax.numpy as jnp
from jax import lax
from jax.experimental import pallas as pl
from jax.experimental.pallas import tpu as pltpu
from jax.sharding import PartitionSpec as P

MESH = pl.DeviceIdType.MESH
BLOCK = 64
NZ, NX, NT = 8, 4, 8
ROWS = 128
WIDTH = 256
HEADS, DH = 4, 64
SEL = 8
FEATS = 128
KB = 2 * NX
NEVER = 1e30
SEMS = 5 * NZ + 4 * NX + NX + NT + NZ + 3 * NX + NZ
F32, BF16 = jnp.float32, jnp.bfloat16

UP, DOWN = NZ // 2, NZ // 2 - 1


def up_slot(s):
    return 2 * s - 1


def down_slot(s):
    return 2 * s if s < NZ // 2 else NZ - 1


OFFSETS = [0] + [None] * (NZ - 1)
for _s in range(1, NZ // 2 + 1):
    OFFSETS[up_slot(_s)] = -_s
for _s in range(1, NZ // 2):
    OFFSETS[down_slot(_s)] = _s
PAIR = [0] + [OFFSETS.index(-o) if -o in OFFSETS else NZ - 1 for o in OFFSETS[1:]]
FAR_FIRST = sorted(range(NZ), key=lambda k: -abs(OFFSETS[k]))


def nt_dot(a, b):
    return lax.dot_general(a, b, (((1,), (1,)), ((), ())), preferred_element_type=F32)


def nn_dot(a, b):
    return lax.dot_general(a, b, (((1,), (0,)), ((), ())), preferred_element_type=F32)


def diagonal_heads(m):
    lane_head = lax.broadcasted_iota(jnp.int32, (DH, WIDTH), 1) // DH
    out = m[(HEADS - 1) * DH :]
    for h in range(HEADS - 1):
        out = jnp.where(lane_head == h, m[h * DH : (h + 1) * DH], out)
    return out


def kernel(
    q_hbm, k_hbm, v_hbm, o_hbm, g_hbm, l_hbm, pick_hbm, n_hbm,
    gq_hbm, gk_hbm, gv_hbm, gw_hbm,
    gk_ref, gv_ref, gw_ref, o_ref, l_ref, pick_ref, n_ref,
    qa, ga, meta, kx, vx, kbd, vbd, kbt, ps, ds, dqs, dqr, dq0,
    nx, nt, ntt, dqx, dks, dvs, dkr, dvr, dk0, dv0, gws, gwr, gw0,
    load_sem, store_sem, send_sem, recv_sem,
):
    kv = lax.axis_index("kv")
    t = lax.axis_index("tp")
    a = kv // NX
    b = kv % NX
    scale = DH**-0.5
    log2e = 1.0 / math.log(2.0)
    scope = jax.named_scope

    def z_of(off):
        return (a + NZ + off) % NZ

    def at_z(off):
        return {"kv": z_of(off) * NX + b, "tp": t}

    def at_x(r):
        return {"kv": a * NX + (b + r) % NX, "tp": t}

    def at_t(r):
        return {"kv": kv, "tp": (t + r) % NT}

    started = []
    counts = [0]

    def sems(n):
        first = counts[0]
        counts[0] += n
        return first

    S_RING = [sems(NZ) for _ in range(5)]
    S_K, S_V = [sems(NX), sems(NX)], [sems(NX), sems(NX)]
    S_N, S_T = sems(NX), sems(NT)
    S_DQ, S_DK, S_DV, S_X, S_W = sems(NZ), sems(NX), sems(NX), sems(NX), sems(NZ)
    assert counts[0] == SEMS

    def send(src, dst, at_mine, at_theirs, dev, keep=True):
        copy = pltpu.make_async_remote_copy(
            src_ref=src, dst_ref=dst, send_sem=send_sem.at[at_mine], recv_sem=recv_sem.at[at_theirs],
            device_id=dev, device_id_type=MESH,
        )
        copy.start()
        if keep:
            started.append(copy)
        return copy

    def arrived(dst, at_mine, dev):
        pltpu.make_async_remote_copy(
            src_ref=dst, dst_ref=dst, send_sem=send_sem.at[at_mine], recv_sem=recv_sem.at[at_mine],
            device_id=dev, device_id_type=MESH,
        ).wait_recv()

    def slot_rows(slot):
        return pl.ds(slot * ROWS, ROWS)

    def half(ref, slot, i):
        return ref.at[pl.ds(slot * ROWS + i * BLOCK, BLOCK), :]

    own_cols = pl.ds(pl.multiple_of(b * FEATS, FEATS), FEATS)
    loads = [
        pltpu.make_async_copy(src, dst, load_sem.at[i])
        for i, (src, dst) in enumerate((
            (q_hbm, qa.at[slot_rows(0), :]), (g_hbm, ga.at[slot_rows(0), :]), (k_hbm, kx.at[0]), (v_hbm, vx.at[0]),
            (o_hbm, o_ref), (l_hbm, l_ref), (pick_hbm, pick_ref), (n_hbm, n_ref), (n_hbm.at[:, own_cols], nx.at[0]),
        ))
    ]
    for copy in loads:
        copy.start()

    barrier = pltpu.get_barrier_semaphore()
    peers = [at_t(r) for r in range(1, NT)] + [at_x(r) for r in range(1, NX)] + [at_z(1), at_z(-1)]
    for dev in peers:
        pl.semaphore_signal(barrier, inc=1, device_id=dev, device_id_type=MESH)
    with scope("load"):
        for copy in loads:
            copy.wait()

    prod = ga[slot_rows(0), :].astype(F32) * o_ref[...].astype(F32)
    high = prod.astype(BF16)
    low = (prod - high.astype(F32)).astype(BF16)
    ones = (
        lax.broadcasted_iota(jnp.int32, (8, WIDTH), 1) // DH == lax.broadcasted_iota(jnp.int32, (8, WIDTH), 0)
    ).astype(BF16)
    dots = nt_dot(ones, high) + nt_dot(ones, low)
    meta[0, 0:HEADS, :] = l_ref[...] * log2e
    meta[0, HEADS : 2 * HEADS, :] = dots[0:HEADS]
    meta[0, 8:16, :] = jnp.full((8, ROWS), -2.0, F32)
    for h in range(HEADS):
        meta[0, 8 + 2 * h : 10 + 2 * h, 0:SEL] = pick_ref[h].astype(F32)

    with scope("barrier"):
        pl.semaphore_wait(barrier, len(peers))

    up_order = [("m", UP), ("q0", UP), ("q1", UP), ("g0", DOWN), ("g1", DOWN)]
    down_order = [("g0", UP), ("g1", UP), ("m", DOWN), ("q0", DOWN), ("q1", DOWN)]
    names = ["m", "q0", "q1", "g0", "g1"]

    def piece_at(name, slot):
        if name == "m":
            return meta.at[slot]
        return half(qa if name[0] == "q" else ga, slot, int(name[1]))

    def ring_step(s):
        for pieces in zip(up_order, down_order):
            for (name, limit), slot_of, to in zip(pieces, (up_slot, down_slot), (1, -1)):
                sem = S_RING[names.index(name)]
                if 0 < s <= limit:
                    arrived(piece_at(name, slot_of(s)), sem + slot_of(s), at_z(-to))
                if s < limit:
                    there = slot_of(s + 1)
                    src = piece_at(name, slot_of(s) if s else 0)
                    send(src, piece_at(name, there), sem + there, sem + there, at_z(to))

    def key_half(ref, r, i):
        return ref.at[r, pl.ds(i * BLOCK, BLOCK), :]

    def send_keys(ref, first, r, i, source=0):
        there = (source - r) % NX
        send(key_half(ref, source, i), key_half(ref, there, i), first[i] + there, first[i] + there, at_x(r))

    def keys_arrived(ref, first, r, i):
        arrived(key_half(ref, r, i), first[i] + r, at_x(r))

    with scope("start"):
        ring_step(0)
        for i in range(2):
            send_keys(kx, S_K, 1, i)
            send_keys(vx, S_V, 3, i)
        for i in range(2):
            send_keys(vx, S_V, 1, i)
            send_keys(kx, S_K, 3, i)
        for r in (1, 3, 2):
            there = (b + r) % NX
            cols = pl.ds(pl.multiple_of(there * FEATS, FEATS), FEATS)
            send(n_ref.at[:, cols], nx.at[NX - r], S_N + r, S_N + NX - r, at_x(r))

    lane_head = lax.broadcasted_iota(jnp.int32, (BLOCK, WIDTH), 1) // DH
    t_head = lax.broadcasted_iota(jnp.int32, (WIDTH, 2 * BLOCK), 0) // DH
    t_half = lax.broadcasted_iota(jnp.int32, (WIDTH, 2 * BLOCK), 1) // BLOCK

    def lay_out_keys(r):
        for i in range(2):
            j = 2 * r + i
            kb = kx[r, i * BLOCK : (i + 1) * BLOCK, :]
            vb = vx[r, i * BLOCK : (i + 1) * BLOCK, :]
            zero = jnp.zeros_like(kb)
            for h in range(HEADS):
                kbd[j, h * DH : (h + 1) * DH, :] = jnp.where(lane_head == h, kb, zero)
                vbd[j, h * DH : (h + 1) * DH, :] = jnp.where(lane_head == h, vb, zero)
            turned = jnp.concatenate([kb, kb], axis=0).T
            for hh in range(HEADS // 2):
                kbt[:, pl.ds(j * WIDTH + hh * ROWS, ROWS)] = jnp.where(
                    t_head == 2 * hh + t_half, turned, jnp.zeros_like(turned)
                )

    with scope("lay0"):
        lay_out_keys(0)

    key_at = lax.broadcasted_iota(jnp.int32, (BLOCK, ROWS), 0)
    row_at = lax.broadcasted_iota(jnp.int32, (BLOCK, ROWS), 1)
    first_block = lax.broadcasted_iota(jnp.int32, (1, ROWS), 1) < BLOCK

    def side_by_side(parts):
        return parts[0] if len(parts) == 1 else jnp.concatenate(parts, axis=1)

    def tile(j, slot, count, own_block=None):
        wide = count * ROWS
        rows = pl.ds(slot * ROWS, wide)
        scores = nt_dot(kbd[j], qa[rows, :])
        gp = nt_dot(vbd[j], ga[rows, :])
        block_id = (a * KB + 2 * ((b + j // 2) % NX) + j % 2).astype(F32)
        hits = [
            jnp.max(jnp.where(meta[slot + c, 8:16, :] == block_id, 1.0, 0.0), axis=1, keepdims=True)
            for c in range(count)
        ]
        for h in range(HEADS):
            offs = []
            for hit, c in zip(hits, range(count)):
                named = jnp.where(first_block, hit[2 * h : 2 * h + 1, :], hit[2 * h + 1 : 2 * h + 2, :]) > 0.5
                offs.append(jnp.where(named, meta[slot + c, h : h + 1, :], NEVER))
            off = side_by_side(offs)
            if own_block is not None:
                ok = key_at <= row_at % BLOCK
                own = jnp.where(ok, jnp.broadcast_to(meta[0, h : h + 1, :], ok.shape), NEVER)
                off = jnp.where(row_at // BLOCK == own_block, own, jnp.broadcast_to(off, ok.shape))
            dots_row = side_by_side([meta[slot + c, HEADS + h : HEADS + h + 1, :] for c in range(count)])
            part = slice(h * DH, (h + 1) * DH)
            p = jnp.exp2(scores[part] * (scale * log2e) - off)
            ps[j, part, pl.ds(slot * ROWS, wide)] = p.astype(BF16)
            ds[pl.ds(j * WIDTH + h * DH, DH), pl.ds(slot * ROWS, wide)] = (p * (gp[part] - dots_row)).astype(BF16)

    def tiles(slot, count, js):
        for j in js:
            tile(j, slot, count)

    def query_grads(slot, count):
        part = nn_dot(kbt[...], ds[:, pl.ds(slot * ROWS, count * ROWS)])
        for c in range(count):
            k = slot + c
            piece = part[:, c * ROWS : (c + 1) * ROWS]
            if k == 0:
                dq0[...] = piece
            else:
                dqs[k] = piece.astype(BF16)
        for c in range(count):
            k = slot + c
            if k:

                @pl.when(z_of(OFFSETS[k]) > a)
                def _(k=k):
                    send(dqs.at[k], dqr.at[PAIR[k]], S_DQ + k, S_DQ + PAIR[k], at_z(OFFSETS[k]), keep=False)

    with scope("own_tiles"):
        for i in range(2):
            tile(i, 0, 1, own_block=i)
    with scope("keys_pass_on"):
        for i in range(2):
            keys_arrived(kx, S_K, 3, i)
            send_keys(kx, S_K, 1, i, source=3)
            keys_arrived(vx, S_V, 1, i)
            send_keys(vx, S_V, 3, i, source=1)
    with scope("ring1"):
        ring_step(1)
    with scope("keys_near"):
        for i in range(2):
            keys_arrived(vx, S_V, 3, i)
            keys_arrived(kx, S_K, 1, i)
        lay_out_keys(1)
        lay_out_keys(3)
    with scope("tiles_a"):
        tiles(1, 2, (0, 1, 2, 3, 6, 7))
        tiles(0, 1, (2, 3, 6, 7))
    with scope("ring2"):
        ring_step(2)
    with scope("keys_far"):
        for i in range(2):
            keys_arrived(kx, S_K, 2, i)
            keys_arrived(vx, S_V, 2, i)
        lay_out_keys(2)
    with scope("nx"):
        for r in (1, 3, 2):
            arrived(nx.at[r], S_N + r, at_x(r))
        for r in range(1, NT):
            send(nx, nt.at[t], S_T + r, S_T + NT - r, at_t(r))
        nt[t] = nx[...]
    with scope("tiles_b"):
        tiles(1, 2, (4, 5))
        query_grads(1, 2)
        tiles(3, 2, range(KB))
        query_grads(3, 2)
    with scope("ring3"):
        ring_step(3)
    with scope("tiles_c"):
        tiles(0, 1, (4, 5))
        query_grads(0, 1)
        tiles(5, 2, range(KB))
        query_grads(5, 2)
    with scope("ring4"):
        ring_step(4)
    with scope("tiles_d"):
        tiles(7, 1, range(KB))
        query_grads(7, 1)

    def key_grads(r):
        for i in range(2):
            j = 2 * r + i
            gv = diagonal_heads(nn_dot(ps[j], ga[...]))
            gk = diagonal_heads(nn_dot(ds[pl.ds(j * WIDTH, WIDTH), :], qa[...])) * scale
            part = slice(i * BLOCK, (i + 1) * BLOCK)
            if r == 0:
                dv0[part, :] = gv
                dk0[part, :] = gk
            else:
                dvs[r, part, :] = gv.astype(BF16)
                dks[r, part, :] = gk.astype(BF16)

    def send_key_grads(r):
        send(dks.at[r], dkr.at[NX - r], S_DK + r, S_DK + NX - r, at_x(r))
        send(dvs.at[r], dvr.at[NX - r], S_DV + r, S_DV + NX - r, at_x(r))

    with scope("key_grads_a"):
        key_grads(2)
        key_grads(1)
    with scope("nt"):
        for r in range(1, NT):
            arrived(nt.at[(t + r) % NT], S_T + r, at_t(r))
        for i, k in enumerate(FAR_FIRST):
            z = z_of(OFFSETS[k])
            for r in range(NX):
                ntt[i * FEATS : (i + 1) * FEATS, r * ROWS : (r + 1) * ROWS] = nt[z, r].T

    with scope("dq_wait"):
        for k in range(1, NZ):

            @pl.when(z_of(OFFSETS[k]) < a)
            def _(k=k):
                arrived(dqr.at[k], S_DQ + k, at_z(OFFSETS[k]))
                dq0[...] += dqr[k].astype(F32)

    with scope("dq_out"):
        dqx[0] = (dq0[...] * scale).T.astype(BF16)
        for r in (2, 1, 3):
            send(dqx.at[0], dqx.at[NX - r], S_X + r, S_X + NX - r, at_x(r))
    stores = [
        pltpu.make_async_copy(src, dst, store_sem.at[i])
        for i, (src, dst) in enumerate(((dqx.at[0], gq_hbm), (gk_ref, gk_hbm), (gv_ref, gv_hbm), (gw_ref, gw_hbm)))
    ]
    stores[0].start()
    send_key_grads(2)
    send_key_grads(1)
    with scope("key_grads_b"):
        key_grads(3)
        send_key_grads(3)
        key_grads(0)

    with scope("dqx"):
        for r in (1, 3, 2):
            arrived(dqx.at[r], S_X + r, at_x(r))
    with scope("gw"):
        dq_row = dqx[...].reshape(NX * ROWS, WIDTH)
        for first in (0, NZ // 2):
            terms = nn_dot(ntt[first * FEATS : (first + NZ // 2) * FEATS, :], dq_row)
            for i, k in enumerate(FAR_FIRST[first : first + NZ // 2]):
                term = terms[i * FEATS : (i + 1) * FEATS]
                if k == 0:
                    gw0[...] = term
                else:
                    gws[k] = term.astype(BF16)
                    send(gws.at[k], gwr.at[PAIR[k]], S_W + k, S_W + PAIR[k], at_z(OFFSETS[k]))

    with scope("dkv_wait"):
        for r in (1, 3, 2):
            arrived(dkr.at[r], S_DK + r, at_x(r))
            arrived(dvr.at[r], S_DV + r, at_x(r))
        sum_k, sum_v = dk0[...], dv0[...]
        for r in range(1, NX):
            sum_k = sum_k + dkr[r].astype(F32)
            sum_v = sum_v + dvr[r].astype(F32)
        gk_ref[...] = sum_k.astype(BF16)
        gv_ref[...] = sum_v.astype(BF16)
        stores[1].start()
        stores[2].start()

    with scope("gw_wait"):
        total_w = gw0[...]
        for k in range(1, NZ):
            arrived(gwr.at[k], S_W + k, at_z(OFFSETS[k]))
        for k in range(1, NZ):
            total_w = total_w + gwr[k].astype(F32)
        gw_ref[...] = total_w
        stores[3].start()
    with scope("end"):
        for k in range(1, NZ):

            @pl.when(z_of(OFFSETS[k]) > a)
            def _(k=k):
                pltpu.make_async_remote_copy(
                    src_ref=dqs.at[k], dst_ref=dqr.at[PAIR[k]], send_sem=send_sem.at[S_DQ + k],
                    recv_sem=recv_sem.at[S_DQ + PAIR[k]], device_id=at_z(OFFSETS[k]), device_id_type=MESH,
                ).wait_send()

        for copy in started:
            copy.wait_send()
        for copy in stores:
            copy.wait()


def put_out(*refs):
    ins, outs, held, sem = refs[:4], refs[4:8], refs[8:12], refs[12]
    loads = [pltpu.make_async_copy(ins[i], held[i], sem.at[i]) for i in range(4)]
    stores = [pltpu.make_async_copy(held[i], outs[i], sem.at[4 + i]) for i in range(4)]
    for copy in loads:
        copy.start()
    for load, store in zip(loads, stores):
        load.wait()
        store.start()
    for copy in stores:
        copy.wait()


def local(queries, keys, values, attended, cotangent, log_totals, block_picks, normed):
    hbm = pl.BlockSpec(memory_space=pltpu.HBM)
    b16 = lambda *shape: pltpu.VMEM(shape, BF16)
    f32 = lambda *shape: pltpu.VMEM(shape, F32)
    shapes = (
        jax.ShapeDtypeStruct((ROWS, WIDTH), BF16),
        jax.ShapeDtypeStruct((ROWS, WIDTH), BF16),
        jax.ShapeDtypeStruct((ROWS, WIDTH), BF16),
        jax.ShapeDtypeStruct((FEATS, WIDTH), F32),
    )
    grads = pl.pallas_call(
        kernel,
        out_shape=shapes,
        in_specs=[hbm] * 8,
        out_specs=(hbm,) * 4,
        scratch_shapes=[
            b16(ROWS, WIDTH), b16(ROWS, WIDTH), f32(FEATS, WIDTH),
            b16(ROWS, WIDTH), f32(HEADS, ROWS), pltpu.VMEM((HEADS, 2, SEL), jnp.int32), b16(ROWS, NX * FEATS),
            b16(NZ * ROWS, WIDTH), b16(NZ * ROWS, WIDTH), f32(NZ, 16, ROWS),
            b16(NX, ROWS, WIDTH), b16(NX, ROWS, WIDTH),
            b16(KB, WIDTH, WIDTH), b16(KB, WIDTH, WIDTH), b16(WIDTH, KB * WIDTH),
            b16(KB, WIDTH, NZ * ROWS), b16(KB * WIDTH, NZ * ROWS),
            b16(NZ, WIDTH, ROWS), b16(NZ, WIDTH, ROWS), f32(WIDTH, ROWS),
            b16(NX, ROWS, FEATS), b16(NT, NX, ROWS, FEATS), b16(NZ * FEATS, NX * ROWS),
            b16(NX, ROWS, WIDTH),
            b16(NX, ROWS, WIDTH), b16(NX, ROWS, WIDTH), b16(NX, ROWS, WIDTH), b16(NX, ROWS, WIDTH),
            f32(ROWS, WIDTH), f32(ROWS, WIDTH),
            b16(NZ, FEATS, WIDTH), b16(NZ, FEATS, WIDTH), f32(FEATS, WIDTH),
            pltpu.SemaphoreType.DMA((9,)),
            pltpu.SemaphoreType.DMA((4,)),
            pltpu.SemaphoreType.DMA((SEMS,)),
            pltpu.SemaphoreType.DMA((SEMS,)),
        ],
        compiler_params=pltpu.CompilerParams(
            collective_id=0, has_side_effects=True, vmem_limit_bytes=67043328
        ),
        name="attention_grads",
    )(queries, keys, values, attended, cotangent, log_totals, block_picks, normed)
    return pl.pallas_call(
        put_out,
        out_shape=shapes,
        in_specs=[hbm] * 4,
        out_specs=(hbm,) * 4,
        scratch_shapes=[*[b16(ROWS, WIDTH)] * 3, f32(FEATS, WIDTH), pltpu.SemaphoreType.DMA((8,))],
        compiler_params=pltpu.CompilerParams(vmem_limit_bytes=67043328),
        name="put_out",
    )(*grads)


def solution(mesh):
    in_specs = (
        P("kv", "tp"),
        P("kv", "tp"),
        P("kv", "tp"),
        P("kv", "tp"),
        P("kv", "tp"),
        P("tp", "kv"),
        P("tp", "kv", None),
        P("kv", "tp"),
    )
    out_specs = (P("kv", "tp"), P("kv", "tp"), P("kv", "tp"), P("kv", "tp"))
    return jax.shard_map(local, mesh=mesh, in_specs=in_specs, out_specs=out_specs, check_vma=False)
```

```python
import functools
import math

import jax
import jax.numpy as jnp
from jax import lax
from jax.experimental import pallas as pl
from jax.experimental.pallas import tpu as pltpu
from jax.sharding import PartitionSpec as P

MESH = pl.DeviceIdType.MESH
BLOCK = 64
NZ, NX, NT = 8, 4, 8
ROWS = 128
WIDTH = 256
HEADS, DH = 4, 64
SEL = 8
FEATS = 128
KB = 2 * NX
NEVER = 1e30
MAIN_VMEM = 67043328 - (3 * 64 + 128) * 1024
SENDS, ARRIVALS = 28, 63
HALF = WIDTH // 2
F32, BF16 = jnp.float32, jnp.bfloat16

UP, DOWN = NZ // 2, NZ // 2 - 1


def up_slot(s):
    return 2 * s - 1


def down_slot(s):
    return 2 * s if s < NZ // 2 else NZ - 1


OFFSETS = [0] + [None] * (NZ - 1)
for _s in range(1, NZ // 2 + 1):
    OFFSETS[up_slot(_s)] = -_s
for _s in range(1, NZ // 2):
    OFFSETS[down_slot(_s)] = _s
PAIR = [0] + [OFFSETS.index(-o) if -o in OFFSETS else NZ - 1 for o in OFFSETS[1:]]
TERMS = (7, 5, 6, 1, 2, 3, 4, 0)


def nt_dot(a, b):
    return lax.dot_general(a, b, (((1,), (1,)), ((), ())), preferred_element_type=F32)


def nn_dot(a, b):
    return lax.dot_general(a, b, (((1,), (0,)), ((), ())), preferred_element_type=F32)


def diagonal_heads(m):
    lane_head = lax.broadcasted_iota(jnp.int32, (DH, WIDTH), 1) // DH
    out = m[(HEADS - 1) * DH :]
    for h in range(HEADS - 1):
        out = jnp.where(lane_head == h, m[h * DH : (h + 1) * DH], out)
    return out


def kernel(
    q_hbm, k_hbm, v_hbm, o_hbm, g_hbm, l_hbm, pick_hbm, n_hbm,
    gq_ref, gk_ref, gv_ref, gw_ref,
    o_ref, l_ref, pick_ref, n_ref,
    qa, ga, meta, offs, kx, vx, kbd, vbd, kbt, ps, ds, dqs, dqr, dq0,
    nx, nt, ntt, dqx, dks, dvs, dkr, dvr, dk0, dv0, gws, gwr, gw3, gw4, gw_own,
    load_sem, send_sem, recv_sem, go_sem,
):
    kv = lax.axis_index("kv")
    t = lax.axis_index("tp")
    a = kv // NX
    b = kv % NX
    scale = DH**-0.5
    log2e = 1.0 / math.log(2.0)
    scope = jax.named_scope

    def z_of(off):
        return (a + NZ + off) % NZ

    def at_z(off):
        return {"kv": z_of(off) * NX + b, "tp": t}

    def at_x(r):
        return {"kv": a * NX + (b + r) % NX, "tp": t}

    def at_t(r):
        return {"kv": kv, "tp": (t + r) % NT}

    counts = [0, 0]

    def take(which, n):
        first = counts[which]
        counts[which] += n
        return first

    def arrivals(n=1):
        return take(1, n)

    class Sends:
        def __init__(self, cond=None):
            self.at, self.cond, self.size = take(0, 1), cond, 0
            groups.append(self)

        def finish(self):
            like = qa if self.size <= 2 * NZ * ROWS * WIDTH else ds
            ref = like.at[pl.ds(0, self.size // (2 * like.shape[1])), :]
            copy = pltpu.make_async_remote_copy(
                src_ref=ref, dst_ref=ref, send_sem=send_sem.at[self.at], recv_sem=recv_sem.at[0],
                device_id=at_x(1), device_id_type=MESH,
            )
            when(self.cond, copy.wait_send)

    groups = []

    S_RING = [arrivals(NZ - 1) - 1 for _ in range(5)]
    S_K = [(arrivals(), arrivals()) if r == 3 else (arrivals(),) * 2 for r in range(1, NX)]
    S_V = [(arrivals(), arrivals()) if r == 1 else (arrivals(),) * 2 for r in range(1, NX)]
    S_N, S_T, S_DQ, S_DK, S_DV, S_X = arrivals(), arrivals(), arrivals(NZ - 1) - 1, arrivals(), arrivals(), arrivals(2)
    S_W3, S_W4, S_W = (arrivals(2), arrivals(2)), arrivals(2), arrivals()

    def when(cond, do):
        if cond is None:
            do()
        else:
            pl.when(cond)(do)

    def send(src, dst, group, at_theirs, dev, counted=False):
        copy = pltpu.make_async_remote_copy(
            src_ref=src, dst_ref=dst, send_sem=send_sem.at[group.at], recv_sem=recv_sem.at[at_theirs],
            device_id=dev, device_id_type=MESH,
        )
        when(group.cond, copy.start)
        group.size += 0 if counted else math.prod(src.shape) * jnp.dtype(src.dtype).itemsize

    def arrived(dst, at_mine, dev):
        pltpu.make_async_remote_copy(
            src_ref=dst, dst_ref=dst, send_sem=send_sem.at[0], recv_sem=recv_sem.at[at_mine],
            device_id=dev, device_id_type=MESH,
        ).wait_recv()

    def slot_rows(slot):
        return pl.ds(slot * ROWS, ROWS)

    def half(ref, slot, i):
        return ref.at[pl.ds(slot * ROWS + i * BLOCK, BLOCK), :]

    own_cols = pl.ds(pl.multiple_of(b * FEATS, FEATS), FEATS)
    loads = [
        pltpu.make_async_copy(src, dst, load_sem.at[i])
        for i, (src, dst) in enumerate((
            (q_hbm, qa.at[slot_rows(0), :]), (g_hbm, ga.at[slot_rows(0), :]), (k_hbm, kx.at[0]), (v_hbm, vx.at[0]),
            (o_hbm, o_ref), (l_hbm, l_ref), (pick_hbm, pick_ref), (n_hbm, n_ref), (n_hbm.at[:, own_cols], nx.at[0]),
        ))
    ]
    for copy in loads:
        copy.start()

    barrier = pltpu.get_barrier_semaphore()
    peers = [at_t(r) for r in range(1, NT)] + [at_x(r) for r in range(1, NX)] + [at_z(1), at_z(-1)]
    for dev in peers:
        pl.semaphore_signal(barrier, inc=1, device_id=dev, device_id_type=MESH)
    with scope("load"):
        for copy in loads:
            copy.wait()

    prod = ga[slot_rows(0), :].astype(F32) * o_ref[...].astype(F32)
    high = prod.astype(BF16)
    low = (prod - high.astype(F32)).astype(BF16)
    ones = (
        lax.broadcasted_iota(jnp.int32, (8, WIDTH), 1) // DH == lax.broadcasted_iota(jnp.int32, (8, WIDTH), 0)
    ).astype(BF16)
    dots = nt_dot(ones, high) + nt_dot(ones, low)
    meta[0, 0:HEADS, :] = l_ref[...] * log2e
    meta[0, HEADS : 2 * HEADS, :] = dots[0:HEADS]
    meta[0, 8:16, :] = jnp.full((8, ROWS), -2.0, F32)
    for h in range(HEADS):
        for c in range(2):
            meta[0, 8 + c * HEADS + h : 9 + c * HEADS + h, 0:SEL] = pick_ref[h, c : c + 1, :].astype(F32)

    first_block = lax.broadcasted_iota(jnp.int32, (HEADS, ROWS), 1) < BLOCK

    def offsets(slot):
        for j in range(KB):
            block_id = (a * KB + 2 * ((b + j // 2) % NX) + j % 2).astype(F32)
            hit = jnp.where(meta[slot, 8:16, :] == block_id, 1.0, 0.0)
            hit = jnp.max(hit, axis=1, keepdims=True)
            named = jnp.where(first_block, hit[0:HEADS], hit[HEADS : 2 * HEADS]) > 0.5
            offs[slot, j, 0:HEADS, :] = jnp.where(named, meta[slot, 0:HEADS, :], NEVER)

    with scope("barrier"):
        pl.semaphore_wait(barrier, len(peers))

    up_order = [("m", UP), ("q0", UP), ("q1", UP), ("g0", DOWN), ("g1", DOWN)]
    down_order = [("g0", UP), ("g1", UP), ("m", DOWN), ("q0", DOWN), ("q1", DOWN)]
    names = ["m", "q0", "q1", "g0", "g1"]

    def piece_at(name, slot):
        if name == "m":
            return meta.at[slot]
        return half(qa if name[0] == "q" else ga, slot, int(name[1]))

    def flows(down, limit, s):
        return a + s < NZ if down else z_of(-s) >= NZ - limit

    def flows_on(down, limit, s):
        return jnp.logical_and(a + s < NZ, a >= 1) if down else z_of(-s) >= NZ - limit

    def clear(ref):
        ref[...] = jnp.zeros(ref.shape, ref.dtype)

    def ring_step(s, between=(), each=2):
        between = list(between)
        sends = {
            (down, limit): Sends(flows_on(down, limit, s)) for down in (False, True) for limit in (UP, DOWN) if s < limit
        }
        for pieces in zip(up_order, down_order):
            for (name, limit), down in zip(pieces, (False, True)):
                sem = S_RING[names.index(name)]
                slot_of, to = (down_slot, -1) if down else (up_slot, 1)
                if 0 < s <= limit:
                    piece, at, comes = piece_at(name, slot_of(s)), sem + slot_of(s), flows(down, limit, s)
                    pl.when(comes)(functools.partial(arrived, piece, at, at_z(-to)))
                    pl.when(jnp.logical_not(comes))(functools.partial(clear, piece))
                    if name == "m":
                        offsets(slot_of(s))
                if s < limit:
                    there = slot_of(s + 1)
                    src = piece_at(name, slot_of(s) if s else 0)
                    send(src, piece_at(name, there), sends[down, limit], sem + there, at_z(to))
            for do in between[:each]:
                do()
            between = between[each:]
        for do in between:
            do()

    def key_half(ref, r, i):
        return ref.at[r, pl.ds(i * BLOCK, BLOCK), :]

    def send_keys(ref, first, r, i, source=0):
        there = (source - r) % NX
        send(key_half(ref, source, i), key_half(ref, there, i), key_sends, first[there - 1][i], at_x(r))

    def key_half_arrived(ref, first, r, i):
        arrived(key_half(ref, r, i), first[r - 1][i], at_x(r))

    def keys_arrived(ref, first, r):
        arrived(ref.at[r], first[r - 1][0], at_x(r))

    key_sends, n_sends, t_sends, x_sends = Sends(), Sends(), Sends(), Sends()
    with scope("start"):
        ring_step(0)
        for i in range(2):
            send_keys(kx, S_K, 1, i)
            send_keys(vx, S_V, 3, i)
        for i in range(2):
            send_keys(vx, S_V, 1, i)
            send_keys(kx, S_K, 3, i)
        for r in (1, 3, 2):
            there = (b + r) % NX
            cols = pl.ds(pl.multiple_of(there * FEATS, FEATS), FEATS)
            send(n_ref.at[:, cols], nx.at[NX - r], n_sends, S_N, at_x(r))

    lane_head = lax.broadcasted_iota(jnp.int32, (BLOCK, WIDTH), 1) // DH
    t_head = lax.broadcasted_iota(jnp.int32, (WIDTH, 2 * BLOCK), 0) // DH
    t_half = lax.broadcasted_iota(jnp.int32, (WIDTH, 2 * BLOCK), 1) // BLOCK

    def lay_out_keys(r):
        for i in range(2):
            j = 2 * r + i
            kb = kx[r, i * BLOCK : (i + 1) * BLOCK, :]
            vb = vx[r, i * BLOCK : (i + 1) * BLOCK, :]
            zero = jnp.zeros_like(kb)
            for h in range(HEADS):
                kbd[j, h * DH : (h + 1) * DH, :] = jnp.where(lane_head == h, kb, zero)
                vbd[j, h * DH : (h + 1) * DH, :] = jnp.where(lane_head == h, vb, zero)
            turned = jnp.concatenate([kb, kb], axis=0).T
            for hh in range(HEADS // 2):
                kbt[:, pl.ds(j * WIDTH + hh * ROWS, ROWS)] = jnp.where(
                    t_head == 2 * hh + t_half, turned, jnp.zeros_like(turned)
                )

    with scope("lay0"):
        lay_out_keys(0)
        offsets(0)

    key_at = lax.broadcasted_iota(jnp.int32, (BLOCK, ROWS), 0)
    row_at = lax.broadcasted_iota(jnp.int32, (BLOCK, ROWS), 1)

    def side_by_side(parts):
        return parts[0] if len(parts) == 1 else jnp.concatenate(parts, axis=1)

    def tile(j, slot, count, own_block=None):
        wide = count * ROWS
        rows = pl.ds(slot * ROWS, wide)
        scores = nt_dot(kbd[j], qa[rows, :])
        gp = nt_dot(vbd[j], ga[rows, :])
        for h in range(HEADS):
            off = side_by_side([offs[slot + c, j, h : h + 1, :] for c in range(count)])
            if own_block is not None:
                ok = key_at <= row_at % BLOCK
                own = jnp.where(ok, jnp.broadcast_to(meta[0, h : h + 1, :], ok.shape), NEVER)
                off = jnp.where(row_at // BLOCK == own_block, own, jnp.broadcast_to(off, ok.shape))
            dots_row = side_by_side([meta[slot + c, HEADS + h : HEADS + h + 1, :] for c in range(count)])
            part = slice(h * DH, (h + 1) * DH)
            p = jnp.exp2(scores[part] * (scale * log2e) - off)
            ps[j, part, pl.ds(slot * ROWS, wide)] = p.astype(BF16)
            ds[pl.ds(j * WIDTH + h * DH, DH), pl.ds(slot * ROWS, wide)] = (p * (gp[part] - dots_row)).astype(BF16)

    def tiles(slot, count, js):
        for j in js:
            tile(j, slot, count)

    def query_grads(slot, count):
        part = nn_dot(kbt[...], ds[:, pl.ds(slot * ROWS, count * ROWS)])
        for c in range(count):
            k = slot + c
            piece = part[:, c * ROWS : (c + 1) * ROWS]
            if k == 0:
                dq0[...] = piece
            else:
                dqs[k] = piece.astype(BF16)

    dq_sends = {k: Sends(z_of(OFFSETS[k]) > a) for k in range(1, NZ)}

    def send_query_grads(*slots, rows=None):
        def start():
            for k in slots:
                send(dqs.at[k], dqr.at[PAIR[k]], dq_sends[k], S_DQ + PAIR[k], at_z(OFFSETS[k]), counted=dq_sends[k].size > 0)

        when(rows, start)

    def key_pass_on(i):
        key_half_arrived(kx, S_K, 3, i)
        send_keys(kx, S_K, 1, i, source=3)
        key_half_arrived(vx, S_V, 1, i)
        send_keys(vx, S_V, 3, i, source=1)

    def spread_normed():
        arrived(nx.at[pl.ds(1, NX - 1)], S_N, at_x(1))
        for r in range(1, NT):
            send(nx, nt.at[t], t_sends, S_T, at_t(r))
        nt[t] = nx[...]

    def lazily(do, *args, **kwargs):
        return functools.partial(do, *args, **kwargs)

    with scope("own_tiles"):
        for i in range(2):
            tile(i, 0, 1, own_block=i)
    with scope("ring1"):
        ring_step(1, [lambda: None, lazily(key_pass_on, 0), lazily(key_pass_on, 1)], 1)
    with scope("keys_near"):
        keys_arrived(vx, S_V, 3)
        keys_arrived(kx, S_K, 1)
        lay_out_keys(1)
        lay_out_keys(3)
    with scope("ring2"):
        def last_keys():
            keys_arrived(kx, S_K, 2)
            keys_arrived(vx, S_V, 2)
            lay_out_keys(2)

        def first_grads():
            tiles(1, 2, (4, 5))
            query_grads(1, 2)
            send_query_grads(1, 2, rows=a >= 3)

        work = [
            lazily(tiles, 0, 1, (2, 3)),
            lambda: (spread_normed(), tiles(0, 1, (6, 7))),
            lazily(tiles, 1, 2, (0, 1, 2)),
            lambda: (tiles(1, 2, (3, 6, 7)), last_keys()),
            first_grads,
        ]
        ring_step(2, work, 1)
    with scope("ring3"):
        def second_grads():
            tiles(3, 2, range(4, KB))
            query_grads(3, 2)
            send_query_grads(3, 4)

        work = [
            lambda: None,
            lazily(tiles, 3, 2, (0, 1, 2, 3)),
            lazily(send_query_grads, 2, 1, rows=a < 3),
            second_grads,
        ]
        ring_step(3, work, 1)
    with scope("tiles_c"):
        tiles(5, 2, range(KB))
        query_grads(5, 2)
        send_query_grads(5, 6)

    def farthest():
        ring_step(4)
        tiles(7, 1, range(KB))

    @pl.when(a < NZ // 2)
    def _():
        with scope("farthest"):
            farthest()

    @pl.when(a >= NZ // 2)
    def _():
        cols = pl.ds(7 * ROWS, ROWS)
        ps[:, :, cols] = jnp.zeros((KB, WIDTH, ROWS), BF16)
        ds[:, cols] = jnp.zeros((KB * WIDTH, ROWS), BF16)

    with scope("farthest_dq"):
        query_grads(7, 1)
        send_query_grads(7)
    with scope("own_rest"):
        tiles(0, 1, (4, 5))
        query_grads(0, 1)

    def key_grads(r):
        for i in range(2):
            j = 2 * r + i
            gv = diagonal_heads(nn_dot(ps[j], ga[...]))
            gk = diagonal_heads(nn_dot(ds[pl.ds(j * WIDTH, WIDTH), :], qa[...])) * scale
            part = slice(i * BLOCK, (i + 1) * BLOCK)
            if r == 0:
                dv0[part, :] = gv
                dk0[part, :] = gk
            else:
                dvs[r, part, :] = gv.astype(BF16)
                dks[r, part, :] = gk.astype(BF16)

    def send_key_grads(r):
        send(dks.at[r], dkr.at[NX - r], dkv_sends, S_DK, at_x(r))
        send(dvs.at[r], dvr.at[NX - r], dkv_sends, S_DV, at_x(r))

    dkv_sends, w_sends, w2_sends = Sends(), Sends(), Sends()

    def key_grads_a():
        key_grads(2)
        key_grads(1)

    def turn_normed():
        arrived(nt.at[pl.ds(0, NT - 1)], S_T, at_t(1))
        for i, k in enumerate(TERMS):
            z = z_of(OFFSETS[k])
            for r in range(NX):
                ntt[i * FEATS : (i + 1) * FEATS, r * ROWS : (r + 1) * ROWS] = nt[z, r].T

    def side_work():
        key_grads_a()
        turn_normed()

    with scope("side_a"):
        pl.when(a >= NZ // 2)(side_work)
    with scope("dq_wait"):
        for k in range(1, NZ):

            @pl.when(z_of(OFFSETS[k]) < a)
            def _(k=k):
                arrived(dqr.at[k], S_DQ + k, at_z(OFFSETS[k]))
                dq0[...] += dqr[k].astype(F32)

    @pl.when(a >= NZ // 2)
    def _():
        for z in range(NZ // 2):
            pl.semaphore_signal(go_sem, inc=1, device_id={"kv": z * NX + b, "tp": t}, device_id_type=MESH)

    with scope("dq_out"):
        grad_q = (dq0[...] * scale).T.astype(BF16)
        for c in range(2):
            dqx[c, 0] = grad_q[:, c * HALF : (c + 1) * HALF]
        for c in range(2):
            for r in (2, 1, 3):
                send(dqx.at[c, 0], dqx.at[c, NX - r], x_sends, S_X + c, at_x(r))
        gq_ref[...] = grad_q
    with scope("side_b"):
        pl.when(a < NZ // 2)(side_work)
        key_grads(3)
        key_grads(0)
    def gw_terms(c):
        dq_row = dqx[c].reshape(NX * ROWS, HALF)
        for first in (0, NZ // 2):
            terms = nn_dot(ntt[first * FEATS : (first + NZ // 2) * FEATS, :], dq_row)
            for i, k in enumerate(TERMS[first : first + NZ // 2]):
                term = terms[i * FEATS : (i + 1) * FEATS]
                if k in (0, 3, 4):
                    gw_own[c, (0, 3, 4).index(k)] = term
                    continue
                gws[c, k] = term.astype(BF16)
                if k == 7:
                    send(gws.at[c, k], gw4.at[c], w_sends, S_W4 + c, at_z(4 * c - 2))
                elif k in (5, 6):
                    send(gws.at[c, k], gw3.at[c, k - 5], w_sends, S_W3[c] + k - 5, at_z(-1 if k == 5 else 1))
                else:
                    send(gws.at[c, k], gwr.at[c, PAIR[k]], w_sends, S_W, at_z(OFFSETS[k]))

    def gw_pass_on(c):
        for side in (1 - c, c):
            k = 3 + side
            arrived(gw3.at[c, side], S_W3[c] + side, at_z(1 - 2 * side))
            term = gw_own[c, 1 + side] + gw3[c, side].astype(F32)
            if side == c:
                arrived(gw4.at[c], S_W4 + c, at_z(2 - 4 * c))
                term = term + gw4[c].astype(F32)
            gws[c, k] = term.astype(BF16)
            send(gws.at[c, k], gwr.at[c, PAIR[k]], w2_sends, S_W, at_z(OFFSETS[k]))

    with scope("go"):

        @pl.when(a < NZ // 2)
        def _():
            pl.semaphore_wait(go_sem, NZ // 2)

    for c in range(2):
        with scope(f"dqx{c}"):
            arrived(dqx.at[c, pl.ds(1, NX - 1)], S_X + c, at_x(1))
        with scope(f"gw{c}"):
            gw_terms(c)
    for r in (2, 1, 3):
        send_key_grads(r)
    for c in range(2):
        with scope(f"gw_pass_on{c}"):
            gw_pass_on(c)

    with scope("dkv_wait"):
        arrived(dkr.at[pl.ds(1, NX - 1)], S_DK, at_x(1))
        arrived(dvr.at[pl.ds(1, NX - 1)], S_DV, at_x(1))
        sum_k, sum_v = dk0[...], dv0[...]
        for r in range(1, NX):
            sum_k = sum_k + dkr[r].astype(F32)
            sum_v = sum_v + dvr[r].astype(F32)
        gk_ref[...] = sum_k.astype(BF16)
        gv_ref[...] = sum_v.astype(BF16)

    with scope("gw_wait"):
        arrived(qa.at[pl.ds(0, 4 * ROWS), :], S_W, at_z(1))
        for c in range(2):
            total_w = gw_own[c, 0]
            for k in range(1, 5):
                total_w = total_w + gwr[c, k].astype(F32)
            gw_ref[:, c * HALF : (c + 1) * HALF] = total_w
    with scope("end"):
        for group in groups:
            group.finish()
        assert counts == [SENDS, ARRIVALS], counts


def put_out(*refs):
    stores = [pltpu.make_async_copy(refs[i], refs[4 + i], refs[8].at[i]) for i in range(4)]
    for copy in stores:
        copy.start()
    for copy in stores:
        copy.wait()


def local(queries, keys, values, attended, cotangent, log_totals, block_picks, normed):
    vmem = pl.BlockSpec(memory_space=pltpu.VMEM)
    hbm = pl.BlockSpec(memory_space=pltpu.HBM)
    b16 = lambda *shape: pltpu.VMEM(shape, BF16)
    f32 = lambda *shape: pltpu.VMEM(shape, F32)
    shapes = (
        jax.ShapeDtypeStruct((ROWS, WIDTH), BF16),
        jax.ShapeDtypeStruct((ROWS, WIDTH), BF16),
        jax.ShapeDtypeStruct((ROWS, WIDTH), BF16),
        jax.ShapeDtypeStruct((FEATS, WIDTH), F32),
    )
    grads = pl.pallas_call(
        kernel,
        out_shape=tuple(pltpu.VMEM(x.shape, x.dtype) for x in shapes),
        in_specs=[hbm] * 8,
        out_specs=(vmem,) * 4,
        scratch_shapes=[
            b16(ROWS, WIDTH), f32(HEADS, ROWS), pltpu.VMEM((HEADS, 2, SEL), jnp.int32), b16(ROWS, NX * FEATS),
            b16(NZ * ROWS, WIDTH), b16(NZ * ROWS, WIDTH), f32(NZ, 16, ROWS), f32(NZ, KB, 8, ROWS),
            b16(NX, ROWS, WIDTH), b16(NX, ROWS, WIDTH),
            b16(KB, WIDTH, WIDTH), b16(KB, WIDTH, WIDTH), b16(WIDTH, KB * WIDTH),
            b16(KB, WIDTH, NZ * ROWS), b16(KB * WIDTH, NZ * ROWS),
            b16(NZ, WIDTH, ROWS), b16(NZ, WIDTH, ROWS), f32(WIDTH, ROWS),
            b16(NX, ROWS, FEATS), b16(NT, NX, ROWS, FEATS), b16(NZ * FEATS, NX * ROWS),
            b16(2, NX, ROWS, HALF),
            b16(NX, ROWS, WIDTH), b16(NX, ROWS, WIDTH), b16(NX, ROWS, WIDTH), b16(NX, ROWS, WIDTH),
            f32(ROWS, WIDTH), f32(ROWS, WIDTH),
            b16(2, NZ, FEATS, HALF), b16(2, 5, FEATS, HALF),
            b16(2, 2, FEATS, HALF), b16(2, FEATS, HALF), f32(2, 3, FEATS, HALF),
            pltpu.SemaphoreType.DMA((9,)),
            pltpu.SemaphoreType.DMA((SENDS,)),
            pltpu.SemaphoreType.DMA((ARRIVALS,)),
            pltpu.SemaphoreType.REGULAR,
        ],
        compiler_params=pltpu.CompilerParams(
            collective_id=0, has_side_effects=True, vmem_limit_bytes=MAIN_VMEM
        ),
        name="attention_grads",
    )(queries, keys, values, attended, cotangent, log_totals, block_picks, normed)
    return pl.pallas_call(
        put_out,
        out_shape=shapes,
        in_specs=[vmem] * 4,
        out_specs=(hbm,) * 4,
        scratch_shapes=[pltpu.SemaphoreType.DMA((4,))],
        compiler_params=pltpu.CompilerParams(vmem_limit_bytes=1024 * 1024),
        name="put_out",
    )(*grads)


def solution(mesh):
    in_specs = (
        P("kv", "tp"),
        P("kv", "tp"),
        P("kv", "tp"),
        P("kv", "tp"),
        P("kv", "tp"),
        P("tp", "kv"),
        P("tp", "kv", None),
        P("kv", "tp"),
    )
    out_specs = (P("kv", "tp"), P("kv", "tp"), P("kv", "tp"), P("kv", "tp"))
    return jax.shard_map(local, mesh=mesh, in_specs=in_specs, out_specs=out_specs, check_vma=False)
```

```python
import functools
import math

import jax
import jax.numpy as jnp
from jax import lax
from jax.experimental import pallas as pl
from jax.experimental.pallas import tpu as pltpu
from jax.sharding import PartitionSpec as P

MESH = pl.DeviceIdType.MESH
BLOCK = 64
NZ, NX, NT = 8, 4, 8
ROWS = 128
WIDTH = 256
HEADS, DH = 4, 64
SEL = 8
FEATS = 128
KB = 2 * NX
NEVER = 1e30
MAIN_VMEM = 67043328 - (3 * 64 + 128) * 1024
SENDS, ARRIVALS = 28, 63
HALF = WIDTH // 2
F32, BF16 = jnp.float32, jnp.bfloat16

UP, DOWN = NZ // 2, NZ // 2 - 1


def up_slot(s):
    return 2 * s - 1


def down_slot(s):
    return 2 * s if s < NZ // 2 else NZ - 1


OFFSETS = [0] + [None] * (NZ - 1)
for _s in range(1, NZ // 2 + 1):
    OFFSETS[up_slot(_s)] = -_s
for _s in range(1, NZ // 2):
    OFFSETS[down_slot(_s)] = _s
PAIR = [0] + [OFFSETS.index(-o) if -o in OFFSETS else NZ - 1 for o in OFFSETS[1:]]
TERMS = (7, 5, 6, 1, 2, 3, 4, 0)


def nt_dot(a, b):
    return lax.dot_general(a, b, (((1,), (1,)), ((), ())), preferred_element_type=F32)


def nn_dot(a, b):
    return lax.dot_general(a, b, (((1,), (0,)), ((), ())), preferred_element_type=F32)


def diagonal_heads(m):
    lane_head = lax.broadcasted_iota(jnp.int32, (DH, WIDTH), 1) // DH
    out = m[(HEADS - 1) * DH :]
    for h in range(HEADS - 1):
        out = jnp.where(lane_head == h, m[h * DH : (h + 1) * DH], out)
    return out


def kernel(
    q_hbm, k_hbm, v_hbm, o_hbm, g_hbm, l_hbm, pick_hbm, n_hbm,
    gq_ref, gk_ref, gv_ref, gw_ref,
    o_ref, l_ref, pick_ref, n_ref,
    qa, ga, meta, offs, kx, vx, kbd, vbd, kbt, ps, ds, dqs, dqr, dq0,
    nx, nt, ntt, dqx, dks, dvs, dkr, dvr, dk0, dv0, gws, gwr, gw3, gw4, gw_own,
    load_sem, send_sem, recv_sem, go_sem,
):
    kv = lax.axis_index("kv")
    t = lax.axis_index("tp")
    a = kv // NX
    b = kv % NX
    scale = DH**-0.5
    log2e = 1.0 / math.log(2.0)
    scope = jax.named_scope

    def z_of(off):
        return (a + NZ + off) % NZ

    def at_z(off):
        return {"kv": z_of(off) * NX + b, "tp": t}

    def at_x(r):
        return {"kv": a * NX + (b + r) % NX, "tp": t}

    def at_t(r):
        return {"kv": kv, "tp": (t + r) % NT}

    counts = [0, 0]

    def take(which, n):
        first = counts[which]
        counts[which] += n
        return first

    def arrivals(n=1):
        return take(1, n)

    class Sends:
        def __init__(self, cond=None):
            self.at, self.cond, self.size = take(0, 1), cond, 0
            groups.append(self)

        def finish(self):
            like = qa if self.size <= 2 * NZ * ROWS * WIDTH else ds
            ref = like.at[pl.ds(0, self.size // (2 * like.shape[1])), :]
            copy = pltpu.make_async_remote_copy(
                src_ref=ref, dst_ref=ref, send_sem=send_sem.at[self.at], recv_sem=recv_sem.at[0],
                device_id=at_x(1), device_id_type=MESH,
            )
            when(self.cond, copy.wait_send)

    groups = []

    S_RING = [arrivals(NZ - 1) - 1 for _ in range(5)]
    S_K = [(arrivals(), arrivals()) if r == 3 else (arrivals(),) * 2 for r in range(1, NX)]
    S_V = [(arrivals(), arrivals()) if r == 1 else (arrivals(),) * 2 for r in range(1, NX)]
    S_N, S_T, S_DQ, S_DK, S_DV, S_X = arrivals(), arrivals(), arrivals(NZ - 1) - 1, arrivals(), arrivals(), arrivals(2)
    S_W3, S_W4, S_W = (arrivals(2), arrivals(2)), arrivals(2), arrivals()

    def when(cond, do):
        if cond is None:
            do()
        else:
            pl.when(cond)(do)

    def send(src, dst, group, at_theirs, dev, counted=False):
        copy = pltpu.make_async_remote_copy(
            src_ref=src, dst_ref=dst, send_sem=send_sem.at[group.at], recv_sem=recv_sem.at[at_theirs],
            device_id=dev, device_id_type=MESH,
        )
        when(group.cond, copy.start)
        group.size += 0 if counted else math.prod(src.shape) * jnp.dtype(src.dtype).itemsize

    def arrived(dst, at_mine, dev):
        pltpu.make_async_remote_copy(
            src_ref=dst, dst_ref=dst, send_sem=send_sem.at[0], recv_sem=recv_sem.at[at_mine],
            device_id=dev, device_id_type=MESH,
        ).wait_recv()

    def slot_rows(slot):
        return pl.ds(slot * ROWS, ROWS)

    def half(ref, slot, i):
        return ref.at[pl.ds(slot * ROWS + i * BLOCK, BLOCK), :]

    own_cols = pl.ds(pl.multiple_of(b * FEATS, FEATS), FEATS)
    loads = [
        pltpu.make_async_copy(src, dst, load_sem.at[i])
        for i, (src, dst) in enumerate((
            (q_hbm, qa.at[slot_rows(0), :]), (g_hbm, ga.at[slot_rows(0), :]), (k_hbm, kx.at[0]), (v_hbm, vx.at[0]),
            (o_hbm, o_ref), (l_hbm, l_ref), (pick_hbm, pick_ref), (n_hbm, n_ref), (n_hbm.at[:, own_cols], nx.at[0]),
        ))
    ]
    for copy in loads:
        copy.start()

    barrier = pltpu.get_barrier_semaphore()
    peers = [at_t(r) for r in range(1, NT)] + [at_x(r) for r in range(1, NX)] + [at_z(1), at_z(-1)]
    for dev in peers:
        pl.semaphore_signal(barrier, inc=1, device_id=dev, device_id_type=MESH)
    with scope("load"):
        for copy in loads:
            copy.wait()

    prod = ga[slot_rows(0), :].astype(F32) * o_ref[...].astype(F32)
    high = prod.astype(BF16)
    low = (prod - high.astype(F32)).astype(BF16)
    ones = (
        lax.broadcasted_iota(jnp.int32, (8, WIDTH), 1) // DH == lax.broadcasted_iota(jnp.int32, (8, WIDTH), 0)
    ).astype(BF16)
    dots = nt_dot(ones, high) + nt_dot(ones, low)
    meta[0, 0:HEADS, :] = l_ref[...] * log2e
    meta[0, HEADS : 2 * HEADS, :] = dots[0:HEADS]
    meta[0, 8:16, :] = jnp.full((8, ROWS), -2.0, F32)
    for h in range(HEADS):
        for c in range(2):
            meta[0, 8 + c * HEADS + h : 9 + c * HEADS + h, 0:SEL] = pick_ref[h, c : c + 1, :].astype(F32)

    first_block = lax.broadcasted_iota(jnp.int32, (HEADS, ROWS), 1) < BLOCK

    def offsets(slot):
        for j in range(KB):
            block_id = (a * KB + 2 * ((b + j // 2) % NX) + j % 2).astype(F32)
            hit = jnp.where(meta[slot, 8:16, :] == block_id, 1.0, 0.0)
            hit = jnp.max(hit, axis=1, keepdims=True)
            named = jnp.where(first_block, hit[0:HEADS], hit[HEADS : 2 * HEADS]) > 0.5
            offs[slot, j, 0:HEADS, :] = jnp.where(named, meta[slot, 0:HEADS, :], NEVER)

    with scope("barrier"):
        pl.semaphore_wait(barrier, len(peers))

    up_order = [("m", UP), ("q0", UP), ("q1", UP), ("g0", DOWN), ("g1", DOWN)]
    down_order = [("g0", UP), ("g1", UP), ("m", DOWN), ("q0", DOWN), ("q1", DOWN)]
    names = ["m", "q0", "q1", "g0", "g1"]

    def piece_at(name, slot):
        if name == "m":
            return meta.at[slot]
        return half(qa if name[0] == "q" else ga, slot, int(name[1]))

    def flows(down, limit, s):
        return a + s < NZ if down else z_of(-s) >= NZ - limit

    def flows_on(down, limit, s):
        return jnp.logical_and(a + s < NZ, a >= 1) if down else z_of(-s) >= NZ - limit

    def clear(ref):
        ref[...] = jnp.zeros(ref.shape, ref.dtype)

    def ring_step(s, between=(), each=2):
        between = list(between)
        sends = {
            (down, limit): Sends(flows_on(down, limit, s)) for down in (False, True) for limit in (UP, DOWN) if s < limit
        }
        for pieces in zip(up_order, down_order):
            for (name, limit), down in zip(pieces, (False, True)):
                sem = S_RING[names.index(name)]
                slot_of, to = (down_slot, -1) if down else (up_slot, 1)
                if 0 < s <= limit:
                    piece, at, comes = piece_at(name, slot_of(s)), sem + slot_of(s), flows(down, limit, s)
                    pl.when(comes)(functools.partial(arrived, piece, at, at_z(-to)))
                    pl.when(jnp.logical_not(comes))(functools.partial(clear, piece))
                    if name == "m":
                        offsets(slot_of(s))
                if s < limit:
                    there = slot_of(s + 1)
                    src = piece_at(name, slot_of(s) if s else 0)
                    send(src, piece_at(name, there), sends[down, limit], sem + there, at_z(to))
            for do in between[:each]:
                do()
            between = between[each:]
        for do in between:
            do()

    def key_half(ref, r, i):
        return ref.at[r, pl.ds(i * BLOCK, BLOCK), :]

    def send_keys(ref, first, r, i, source=0):
        there = (source - r) % NX
        send(key_half(ref, source, i), key_half(ref, there, i), key_sends, first[there - 1][i], at_x(r))

    def key_half_arrived(ref, first, r, i):
        arrived(key_half(ref, r, i), first[r - 1][i], at_x(r))

    def keys_arrived(ref, first, r):
        arrived(ref.at[r], first[r - 1][0], at_x(r))

    key_sends, n_sends, t_sends, x_sends = Sends(), Sends(), Sends(), Sends()
    with scope("start"):
        ring_step(0)
        for i in range(2):
            send_keys(kx, S_K, 1, i)
            send_keys(vx, S_V, 3, i)
        for i in range(2):
            send_keys(vx, S_V, 1, i)
            send_keys(kx, S_K, 3, i)
        for r in (1, 3, 2):
            there = (b + r) % NX
            cols = pl.ds(pl.multiple_of(there * FEATS, FEATS), FEATS)
            send(n_ref.at[:, cols], nx.at[NX - r], n_sends, S_N, at_x(r))

    lane_head = lax.broadcasted_iota(jnp.int32, (BLOCK, WIDTH), 1) // DH
    t_head = lax.broadcasted_iota(jnp.int32, (WIDTH, 2 * BLOCK), 0) // DH
    t_half = lax.broadcasted_iota(jnp.int32, (WIDTH, 2 * BLOCK), 1) // BLOCK

    def lay_out_keys(r):
        for i in range(2):
            j = 2 * r + i
            kb = kx[r, i * BLOCK : (i + 1) * BLOCK, :]
            vb = vx[r, i * BLOCK : (i + 1) * BLOCK, :]
            zero = jnp.zeros_like(kb)
            for h in range(HEADS):
                kbd[j, h * DH : (h + 1) * DH, :] = jnp.where(lane_head == h, kb, zero)
                vbd[j, h * DH : (h + 1) * DH, :] = jnp.where(lane_head == h, vb, zero)
            turned = jnp.concatenate([kb, kb], axis=0).T
            for hh in range(HEADS // 2):
                kbt[:, pl.ds(j * WIDTH + hh * ROWS, ROWS)] = jnp.where(
                    t_head == 2 * hh + t_half, turned, jnp.zeros_like(turned)
                )

    with scope("lay0"):
        lay_out_keys(0)
        offsets(0)

    key_at = lax.broadcasted_iota(jnp.int32, (BLOCK, ROWS), 0)
    row_at = lax.broadcasted_iota(jnp.int32, (BLOCK, ROWS), 1)

    def side_by_side(parts):
        return parts[0] if len(parts) == 1 else jnp.concatenate(parts, axis=1)

    def tile(j, slot, count, own_block=None):
        wide = count * ROWS
        rows = pl.ds(slot * ROWS, wide)
        scores = nt_dot(kbd[j], qa[rows, :])
        gp = nt_dot(vbd[j], ga[rows, :])
        for h in range(HEADS):
            off = side_by_side([offs[slot + c, j, h : h + 1, :] for c in range(count)])
            if own_block is not None:
                ok = key_at <= row_at % BLOCK
                own = jnp.where(ok, jnp.broadcast_to(meta[0, h : h + 1, :], ok.shape), NEVER)
                off = jnp.where(row_at // BLOCK == own_block, own, jnp.broadcast_to(off, ok.shape))
            dots_row = side_by_side([meta[slot + c, HEADS + h : HEADS + h + 1, :] for c in range(count)])
            part = slice(h * DH, (h + 1) * DH)
            p = jnp.exp2(scores[part] * (scale * log2e) - off)
            ps[j, part, pl.ds(slot * ROWS, wide)] = p.astype(BF16)
            ds[pl.ds(j * WIDTH + h * DH, DH), pl.ds(slot * ROWS, wide)] = (p * (gp[part] - dots_row)).astype(BF16)

    def tiles(slot, count, js):
        for j in js:
            tile(j, slot, count)

    def query_grads(slot, count):
        part = nn_dot(kbt[...], ds[:, pl.ds(slot * ROWS, count * ROWS)])
        for c in range(count):
            k = slot + c
            piece = part[:, c * ROWS : (c + 1) * ROWS]
            if k == 0:
                dq0[...] = piece
            else:
                dqs[k] = piece.astype(BF16)

    dq_sends = {k: Sends(z_of(OFFSETS[k]) > a) for k in range(1, NZ)}

    def send_query_grads(*slots, rows=None):
        def start():
            for k in slots:
                send(dqs.at[k], dqr.at[PAIR[k]], dq_sends[k], S_DQ + PAIR[k], at_z(OFFSETS[k]), counted=dq_sends[k].size > 0)

        when(rows, start)

    def key_pass_on(i):
        key_half_arrived(kx, S_K, 3, i)
        send_keys(kx, S_K, 1, i, source=3)
        key_half_arrived(vx, S_V, 1, i)
        send_keys(vx, S_V, 3, i, source=1)

    def spread_normed():
        arrived(nx.at[pl.ds(1, NX - 1)], S_N, at_x(1))
        for r in range(1, NT):
            send(nx, nt.at[t], t_sends, S_T, at_t(r))
        nt[t] = nx[...]

    def lazily(do, *args, **kwargs):
        return functools.partial(do, *args, **kwargs)

    with scope("own_tiles"):
        for i in range(2):
            tile(i, 0, 1, own_block=i)
    with scope("ring1"):
        ring_step(1, [lambda: None, lazily(key_pass_on, 0), lazily(key_pass_on, 1)], 1)
    with scope("keys_near"):
        keys_arrived(vx, S_V, 3)
        keys_arrived(kx, S_K, 1)
        lay_out_keys(1)
        lay_out_keys(3)
    with scope("ring2"):
        def last_keys():
            keys_arrived(kx, S_K, 2)
            keys_arrived(vx, S_V, 2)
            lay_out_keys(2)

        def first_grads():
            tiles(1, 2, (4, 5))
            query_grads(1, 2)
            send_query_grads(1, 2, rows=a >= 3)

        work = [
            lazily(tiles, 0, 1, (2, 3)),
            lambda: (spread_normed(), tiles(0, 1, (6, 7))),
            lazily(tiles, 1, 2, (0, 1, 2)),
            lambda: (tiles(1, 2, (3, 6, 7)), last_keys()),
            first_grads,
        ]
        ring_step(2, work, 1)
    with scope("ring3"):
        def second_tiles(js):
            tiles(3, 2, js)

        def second_grads(js):
            tiles(3, 2, js)
            query_grads(3, 2)

        def if_early(do, *args):
            pl.when(a < 3)(functools.partial(do, *args))

        @pl.when(a >= 3)
        def _():
            second_grads(range(KB))
            send_query_grads(4, 3)

        work = [
            lambda: None,
            lazily(if_early, second_tiles, range(4)),
            lazily(send_query_grads, 2, 1, rows=a < 3),
            lambda: (if_early(second_grads, range(4, KB)), send_query_grads(4, 3, rows=a < 3)),
        ]
        ring_step(3, work, 1)
    with scope("tiles_c"):
        tiles(5, 2, range(KB))
        query_grads(5, 2)
        send_query_grads(5, 6)

    def farthest():
        ring_step(4)
        tiles(7, 1, range(KB))

    @pl.when(a < NZ // 2)
    def _():
        with scope("farthest"):
            farthest()

    @pl.when(a >= NZ // 2)
    def _():
        cols = pl.ds(7 * ROWS, ROWS)
        ps[:, :, cols] = jnp.zeros((KB, WIDTH, ROWS), BF16)
        ds[:, cols] = jnp.zeros((KB * WIDTH, ROWS), BF16)

    with scope("farthest_dq"):
        query_grads(7, 1)
        send_query_grads(7)
    with scope("own_rest"):
        tiles(0, 1, (4, 5))
        query_grads(0, 1)

    def key_grads(r):
        for i in range(2):
            j = 2 * r + i
            gv = diagonal_heads(nn_dot(ps[j], ga[...]))
            gk = diagonal_heads(nn_dot(ds[pl.ds(j * WIDTH, WIDTH), :], qa[...])) * scale
            part = slice(i * BLOCK, (i + 1) * BLOCK)
            if r == 0:
                dv0[part, :] = gv
                dk0[part, :] = gk
            else:
                dvs[r, part, :] = gv.astype(BF16)
                dks[r, part, :] = gk.astype(BF16)

    def send_key_grads(r):
        send(dks.at[r], dkr.at[NX - r], dkv_sends, S_DK, at_x(r))
        send(dvs.at[r], dvr.at[NX - r], dkv_sends, S_DV, at_x(r))

    dkv_sends, w_sends, w2_sends = Sends(), Sends(), Sends()

    def key_grads_a():
        key_grads(2)
        key_grads(1)

    def turn_normed():
        arrived(nt.at[pl.ds(0, NT - 1)], S_T, at_t(1))
        for i, k in enumerate(TERMS):
            z = z_of(OFFSETS[k])
            for r in range(NX):
                ntt[i * FEATS : (i + 1) * FEATS, r * ROWS : (r + 1) * ROWS] = nt[z, r].T

    def side_work():
        key_grads_a()
        turn_normed()

    with scope("side_a"):
        pl.when(a >= NZ // 2)(side_work)
    with scope("dq_wait"):
        for k in range(1, NZ):

            @pl.when(z_of(OFFSETS[k]) < a)
            def _(k=k):
                arrived(dqr.at[k], S_DQ + k, at_z(OFFSETS[k]))
                dq0[...] += dqr[k].astype(F32)

    @pl.when(a >= NZ // 2)
    def _():
        for z in range(NZ // 2):
            pl.semaphore_signal(go_sem, inc=1, device_id={"kv": z * NX + b, "tp": t}, device_id_type=MESH)

    with scope("dq_out"):
        grad_q = (dq0[...] * scale).T.astype(BF16)
        for c in range(2):
            dqx[c, 0] = grad_q[:, c * HALF : (c + 1) * HALF]
        for c in range(2):
            for r in (2, 1, 3):
                send(dqx.at[c, 0], dqx.at[c, NX - r], x_sends, S_X + c, at_x(r))
        gq_ref[...] = grad_q
    with scope("side_b"):
        pl.when(a < NZ // 2)(side_work)
        key_grads(3)
        key_grads(0)
    def gw_terms(c):
        dq_row = dqx[c].reshape(NX * ROWS, HALF)
        for first in (0, NZ // 2):
            terms = nn_dot(ntt[first * FEATS : (first + NZ // 2) * FEATS, :], dq_row)
            for i, k in enumerate(TERMS[first : first + NZ // 2]):
                term = terms[i * FEATS : (i + 1) * FEATS]
                if k in (0, 3, 4):
                    gw_own[c, (0, 3, 4).index(k)] = term
                    continue
                gws[c, k] = term.astype(BF16)
                if k == 7:
                    send(gws.at[c, k], gw4.at[c], w_sends, S_W4 + c, at_z(4 * c - 2))
                elif k in (5, 6):
                    send(gws.at[c, k], gw3.at[c, k - 5], w_sends, S_W3[c] + k - 5, at_z(-1 if k == 5 else 1))
                else:
                    send(gws.at[c, k], gwr.at[c, PAIR[k]], w_sends, S_W, at_z(OFFSETS[k]))

    def gw_pass_on(c):
        for side in (1 - c, c):
            k = 3 + side
            arrived(gw3.at[c, side], S_W3[c] + side, at_z(1 - 2 * side))
            term = gw_own[c, 1 + side] + gw3[c, side].astype(F32)
            if side == c:
                arrived(gw4.at[c], S_W4 + c, at_z(2 - 4 * c))
                term = term + gw4[c].astype(F32)
            gws[c, k] = term.astype(BF16)
            send(gws.at[c, k], gwr.at[c, PAIR[k]], w2_sends, S_W, at_z(OFFSETS[k]))

    with scope("go"):

        @pl.when(a < NZ // 2)
        def _():
            pl.semaphore_wait(go_sem, NZ // 2)

    for c in range(2):
        with scope(f"dqx{c}"):
            arrived(dqx.at[c, pl.ds(1, NX - 1)], S_X + c, at_x(1))
        with scope(f"gw{c}"):
            gw_terms(c)
    for r in (2, 1, 3):
        send_key_grads(r)
    for c in range(2):
        with scope(f"gw_pass_on{c}"):
            gw_pass_on(c)

    with scope("dkv_wait"):
        arrived(dkr.at[pl.ds(1, NX - 1)], S_DK, at_x(1))
        arrived(dvr.at[pl.ds(1, NX - 1)], S_DV, at_x(1))
        sum_k, sum_v = dk0[...], dv0[...]
        for r in range(1, NX):
            sum_k = sum_k + dkr[r].astype(F32)
            sum_v = sum_v + dvr[r].astype(F32)
        gk_ref[...] = sum_k.astype(BF16)
        gv_ref[...] = sum_v.astype(BF16)

    with scope("gw_wait"):
        arrived(qa.at[pl.ds(0, 4 * ROWS), :], S_W, at_z(1))
        for c in range(2):
            total_w = gw_own[c, 0]
            for k in range(1, 5):
                total_w = total_w + gwr[c, k].astype(F32)
            gw_ref[:, c * HALF : (c + 1) * HALF] = total_w
    with scope("end"):
        for group in groups:
            group.finish()
        assert counts == [SENDS, ARRIVALS], counts


def put_out(*refs):
    stores = [pltpu.make_async_copy(refs[i], refs[4 + i], refs[8].at[i]) for i in range(4)]
    for copy in stores:
        copy.start()
    for copy in stores:
        copy.wait()


def local(queries, keys, values, attended, cotangent, log_totals, block_picks, normed):
    vmem = pl.BlockSpec(memory_space=pltpu.VMEM)
    hbm = pl.BlockSpec(memory_space=pltpu.HBM)
    b16 = lambda *shape: pltpu.VMEM(shape, BF16)
    f32 = lambda *shape: pltpu.VMEM(shape, F32)
    shapes = (
        jax.ShapeDtypeStruct((ROWS, WIDTH), BF16),
        jax.ShapeDtypeStruct((ROWS, WIDTH), BF16),
        jax.ShapeDtypeStruct((ROWS, WIDTH), BF16),
        jax.ShapeDtypeStruct((FEATS, WIDTH), F32),
    )
    grads = pl.pallas_call(
        kernel,
        out_shape=tuple(pltpu.VMEM(x.shape, x.dtype) for x in shapes),
        in_specs=[hbm] * 8,
        out_specs=(vmem,) * 4,
        scratch_shapes=[
            b16(ROWS, WIDTH), f32(HEADS, ROWS), pltpu.VMEM((HEADS, 2, SEL), jnp.int32), b16(ROWS, NX * FEATS),
            b16(NZ * ROWS, WIDTH), b16(NZ * ROWS, WIDTH), f32(NZ, 16, ROWS), f32(NZ, KB, 8, ROWS),
            b16(NX, ROWS, WIDTH), b16(NX, ROWS, WIDTH),
            b16(KB, WIDTH, WIDTH), b16(KB, WIDTH, WIDTH), b16(WIDTH, KB * WIDTH),
            b16(KB, WIDTH, NZ * ROWS), b16(KB * WIDTH, NZ * ROWS),
            b16(NZ, WIDTH, ROWS), b16(NZ, WIDTH, ROWS), f32(WIDTH, ROWS),
            b16(NX, ROWS, FEATS), b16(NT, NX, ROWS, FEATS), b16(NZ * FEATS, NX * ROWS),
            b16(2, NX, ROWS, HALF),
            b16(NX, ROWS, WIDTH), b16(NX, ROWS, WIDTH), b16(NX, ROWS, WIDTH), b16(NX, ROWS, WIDTH),
            f32(ROWS, WIDTH), f32(ROWS, WIDTH),
            b16(2, NZ, FEATS, HALF), b16(2, 5, FEATS, HALF),
            b16(2, 2, FEATS, HALF), b16(2, FEATS, HALF), f32(2, 3, FEATS, HALF),
            pltpu.SemaphoreType.DMA((9,)),
            pltpu.SemaphoreType.DMA((SENDS,)),
            pltpu.SemaphoreType.DMA((ARRIVALS,)),
            pltpu.SemaphoreType.REGULAR,
        ],
        compiler_params=pltpu.CompilerParams(
            collective_id=0, has_side_effects=True, vmem_limit_bytes=MAIN_VMEM
        ),
        name="attention_grads",
    )(queries, keys, values, attended, cotangent, log_totals, block_picks, normed)
    return pl.pallas_call(
        put_out,
        out_shape=shapes,
        in_specs=[vmem] * 4,
        out_specs=(hbm,) * 4,
        scratch_shapes=[pltpu.SemaphoreType.DMA((4,))],
        compiler_params=pltpu.CompilerParams(vmem_limit_bytes=1024 * 1024),
        name="put_out",
    )(*grads)


def solution(mesh):
    in_specs = (
        P("kv", "tp"),
        P("kv", "tp"),
        P("kv", "tp"),
        P("kv", "tp"),
        P("kv", "tp"),
        P("tp", "kv"),
        P("tp", "kv", None),
        P("kv", "tp"),
    )
    out_specs = (P("kv", "tp"), P("kv", "tp"), P("kv", "tp"), P("kv", "tp"))
    return jax.shard_map(local, mesh=mesh, in_specs=in_specs, out_specs=out_specs, check_vma=False)
```

```python
import functools
import math

import jax
import jax.numpy as jnp
from jax import lax
from jax.experimental import pallas as pl
from jax.experimental.pallas import tpu as pltpu
from jax.sharding import PartitionSpec as P

MESH = pl.DeviceIdType.MESH
BLOCK = 64
NZ, NX, NT = 8, 4, 8
ROWS = 128
WIDTH = 256
HEADS, DH = 4, 64
SEL = 8
FEATS = 128
KB = 2 * NX
NEVER = 1e30
MAIN_VMEM = 67043328 - (3 * 64 + 128) * 1024
SENDS, ARRIVALS = 28, 64
HALF = WIDTH // 2
F32, BF16 = jnp.float32, jnp.bfloat16

UP, DOWN = NZ // 2, NZ // 2 - 1


def up_slot(s):
    return 2 * s - 1


def down_slot(s):
    return 2 * s if s < NZ // 2 else NZ - 1


OFFSETS = [0] + [None] * (NZ - 1)
for _s in range(1, NZ // 2 + 1):
    OFFSETS[up_slot(_s)] = -_s
for _s in range(1, NZ // 2):
    OFFSETS[down_slot(_s)] = _s
PAIR = [0] + [OFFSETS.index(-o) if -o in OFFSETS else NZ - 1 for o in OFFSETS[1:]]
TERMS = (7, 6, 5, 2, 1, 3, 4, 0)


def nt_dot(a, b):
    return lax.dot_general(a, b, (((1,), (1,)), ((), ())), preferred_element_type=F32)


def nn_dot(a, b):
    return lax.dot_general(a, b, (((1,), (0,)), ((), ())), preferred_element_type=F32)


def diagonal_heads(m):
    lane_head = lax.broadcasted_iota(jnp.int32, (DH, WIDTH), 1) // DH
    out = m[(HEADS - 1) * DH :]
    for h in range(HEADS - 1):
        out = jnp.where(lane_head == h, m[h * DH : (h + 1) * DH], out)
    return out


def kernel(
    q_hbm, k_hbm, v_hbm, o_hbm, g_hbm, l_hbm, pick_hbm, n_hbm,
    gq_ref, gk_ref, gv_ref, gw_ref,
    o_ref, l_ref, pick_ref, n_ref,
    qa, ga, meta, offs, kx, vx, kbd, vbd, kbt, ps, ds, dqs, dqr, dqm, dq0,
    nx, nt, ntt, dqx, dks, dvs, dkr, dvr, dk0, dv0, gws, gwr, gw3, gw4, gw_own,
    load_sem, send_sem, recv_sem, go_sem,
):
    kv = lax.axis_index("kv")
    t = lax.axis_index("tp")
    a = kv // NX
    b = kv % NX
    scale = DH**-0.5
    log2e = 1.0 / math.log(2.0)
    scope = jax.named_scope

    def z_of(off):
        return (a + NZ + off) % NZ

    def at_z(off):
        return {"kv": z_of(off) * NX + b, "tp": t}

    def at_x(r):
        return {"kv": a * NX + (b + r) % NX, "tp": t}

    def at_t(r):
        return {"kv": kv, "tp": (t + r) % NT}

    counts = [0, 0]

    def take(which, n):
        first = counts[which]
        counts[which] += n
        return first

    def arrivals(n=1):
        return take(1, n)

    class Sends:
        def __init__(self, cond=None):
            self.at, self.cond, self.size = take(0, 1), cond, 0
            groups.append(self)

        def finish(self):
            like = qa if self.size <= 2 * NZ * ROWS * WIDTH else ds
            ref = like.at[pl.ds(0, self.size // (2 * like.shape[1])), :]
            copy = pltpu.make_async_remote_copy(
                src_ref=ref, dst_ref=ref, send_sem=send_sem.at[self.at], recv_sem=recv_sem.at[0],
                device_id=at_x(1), device_id_type=MESH,
            )
            when(self.cond, copy.wait_send)

    groups = []

    S_RING = [arrivals(NZ - 1) - 1 for _ in range(5)]
    S_K = [(arrivals(), arrivals()) if r == 3 else (arrivals(),) * 2 for r in range(1, NX)]
    S_V = [(arrivals(), arrivals()) if r == 1 else (arrivals(),) * 2 for r in range(1, NX)]
    S_N, S_T, S_DQ, S_DK, S_DV, S_X = arrivals(), arrivals(), arrivals(NZ - 1) - 1, arrivals(), arrivals(), arrivals(2)
    S_DM = arrivals()
    S_W3, S_W4, S_W = (arrivals(2), arrivals(2)), arrivals(2), arrivals()

    def when(cond, do):
        if cond is None:
            do()
        else:
            pl.when(cond)(do)

    def send(src, dst, group, at_theirs, dev, counted=False):
        copy = pltpu.make_async_remote_copy(
            src_ref=src, dst_ref=dst, send_sem=send_sem.at[group.at], recv_sem=recv_sem.at[at_theirs],
            device_id=dev, device_id_type=MESH,
        )
        when(group.cond, copy.start)
        group.size += 0 if counted else math.prod(src.shape) * jnp.dtype(src.dtype).itemsize

    def arrived(dst, at_mine, dev):
        pltpu.make_async_remote_copy(
            src_ref=dst, dst_ref=dst, send_sem=send_sem.at[0], recv_sem=recv_sem.at[at_mine],
            device_id=dev, device_id_type=MESH,
        ).wait_recv()

    def slot_rows(slot):
        return pl.ds(slot * ROWS, ROWS)

    def half(ref, slot, i):
        return ref.at[pl.ds(slot * ROWS + i * BLOCK, BLOCK), :]

    own_cols = pl.ds(pl.multiple_of(b * FEATS, FEATS), FEATS)
    loads = [
        pltpu.make_async_copy(src, dst, load_sem.at[i])
        for i, (src, dst) in enumerate((
            (q_hbm, qa.at[slot_rows(0), :]), (g_hbm, ga.at[slot_rows(0), :]), (k_hbm, kx.at[0]), (v_hbm, vx.at[0]),
            (o_hbm, o_ref), (l_hbm, l_ref), (pick_hbm, pick_ref), (n_hbm, n_ref), (n_hbm.at[:, own_cols], nx.at[0]),
        ))
    ]
    for copy in loads:
        copy.start()

    barrier = pltpu.get_barrier_semaphore()
    peers = [at_t(r) for r in range(1, NT)] + [at_x(r) for r in range(1, NX)] + [at_z(1), at_z(-1)]
    for dev in peers:
        pl.semaphore_signal(barrier, inc=1, device_id=dev, device_id_type=MESH)
    with scope("load"):
        for copy in loads:
            copy.wait()

    prod = ga[slot_rows(0), :].astype(F32) * o_ref[...].astype(F32)
    high = prod.astype(BF16)
    low = (prod - high.astype(F32)).astype(BF16)
    ones = (
        lax.broadcasted_iota(jnp.int32, (8, WIDTH), 1) // DH == lax.broadcasted_iota(jnp.int32, (8, WIDTH), 0)
    ).astype(BF16)
    dots = nt_dot(ones, high) + nt_dot(ones, low)
    meta[0, 0:HEADS, :] = l_ref[...] * log2e
    meta[0, HEADS : 2 * HEADS, :] = dots[0:HEADS]
    meta[0, 8:16, :] = jnp.full((8, ROWS), -2.0, F32)
    for h in range(HEADS):
        for c in range(2):
            meta[0, 8 + c * HEADS + h : 9 + c * HEADS + h, 0:SEL] = pick_ref[h, c : c + 1, :].astype(F32)

    first_block = lax.broadcasted_iota(jnp.int32, (HEADS, ROWS), 1) < BLOCK

    def offsets(slot):
        for j in range(KB):
            block_id = (a * KB + 2 * ((b + j // 2) % NX) + j % 2).astype(F32)
            hit = jnp.where(meta[slot, 8:16, :] == block_id, 1.0, 0.0)
            hit = jnp.max(hit, axis=1, keepdims=True)
            named = jnp.where(first_block, hit[0:HEADS], hit[HEADS : 2 * HEADS]) > 0.5
            offs[slot, j, 0:HEADS, :] = jnp.where(named, meta[slot, 0:HEADS, :], NEVER)

    with scope("barrier"):
        pl.semaphore_wait(barrier, len(peers))

    up_order = [("m", UP), ("q0", UP), ("q1", UP), ("g0", DOWN), ("g1", DOWN)]
    down_order = [("g0", UP), ("g1", UP), ("m", DOWN), ("q0", DOWN), ("q1", DOWN)]
    names = ["m", "q0", "q1", "g0", "g1"]

    def piece_at(name, slot):
        if name == "m":
            return meta.at[slot]
        return half(qa if name[0] == "q" else ga, slot, int(name[1]))

    def flows(down, limit, s):
        return a + s < NZ if down else z_of(-s) >= NZ - limit

    def flows_on(down, limit, s):
        return jnp.logical_and(a + s < NZ, a >= 1) if down else z_of(-s) >= NZ - limit

    def clear(ref):
        ref[...] = jnp.zeros(ref.shape, ref.dtype)

    def ring_step(s, between=(), each=2):
        between = list(between)
        sends = {
            (down, limit): Sends(flows_on(down, limit, s)) for down in (False, True) for limit in (UP, DOWN) if s < limit
        }
        for pieces in zip(up_order, down_order):
            for (name, limit), down in zip(pieces, (False, True)):
                sem = S_RING[names.index(name)]
                slot_of, to = (down_slot, -1) if down else (up_slot, 1)
                if 0 < s <= limit:
                    piece, at, comes = piece_at(name, slot_of(s)), sem + slot_of(s), flows(down, limit, s)
                    pl.when(comes)(functools.partial(arrived, piece, at, at_z(-to)))
                    pl.when(jnp.logical_not(comes))(functools.partial(clear, piece))
                    if name == "m":
                        offsets(slot_of(s))
                if s < limit:
                    there = slot_of(s + 1)
                    src = piece_at(name, slot_of(s) if s else 0)
                    send(src, piece_at(name, there), sends[down, limit], sem + there, at_z(to))
            for do in between[:each]:
                do()
            between = between[each:]
        for do in between:
            do()

    def key_half(ref, r, i):
        return ref.at[r, pl.ds(i * BLOCK, BLOCK), :]

    def send_keys(ref, first, r, i, source=0):
        there = (source - r) % NX
        send(key_half(ref, source, i), key_half(ref, there, i), key_sends, first[there - 1][i], at_x(r))

    def key_half_arrived(ref, first, r, i):
        arrived(key_half(ref, r, i), first[r - 1][i], at_x(r))

    def keys_arrived(ref, first, r):
        arrived(ref.at[r], first[r - 1][0], at_x(r))

    key_sends, n_sends, t_sends, x_sends = Sends(), Sends(), Sends(), Sends()
    with scope("start"):
        ring_step(0)
        for i in range(2):
            send_keys(kx, S_K, 1, i)
            send_keys(vx, S_V, 3, i)
        for i in range(2):
            send_keys(vx, S_V, 1, i)
            send_keys(kx, S_K, 3, i)
        for r in (1, 3, 2):
            there = (b + r) % NX
            cols = pl.ds(pl.multiple_of(there * FEATS, FEATS), FEATS)
            send(n_ref.at[:, cols], nx.at[NX - r], n_sends, S_N, at_x(r))

    lane_head = lax.broadcasted_iota(jnp.int32, (BLOCK, WIDTH), 1) // DH
    t_head = lax.broadcasted_iota(jnp.int32, (WIDTH, 2 * BLOCK), 0) // DH
    t_half = lax.broadcasted_iota(jnp.int32, (WIDTH, 2 * BLOCK), 1) // BLOCK

    def lay_out_keys(r):
        for i in range(2):
            j = 2 * r + i
            kb = kx[r, i * BLOCK : (i + 1) * BLOCK, :]
            vb = vx[r, i * BLOCK : (i + 1) * BLOCK, :]
            zero = jnp.zeros_like(kb)
            for h in range(HEADS):
                kbd[j, h * DH : (h + 1) * DH, :] = jnp.where(lane_head == h, kb, zero)
                vbd[j, h * DH : (h + 1) * DH, :] = jnp.where(lane_head == h, vb, zero)
            turned = jnp.concatenate([kb, kb], axis=0).T
            for hh in range(HEADS // 2):
                kbt[:, pl.ds(j * WIDTH + hh * ROWS, ROWS)] = jnp.where(
                    t_head == 2 * hh + t_half, turned, jnp.zeros_like(turned)
                )

    with scope("lay0"):
        lay_out_keys(0)
        offsets(0)

    key_at = lax.broadcasted_iota(jnp.int32, (BLOCK, ROWS), 0)
    row_at = lax.broadcasted_iota(jnp.int32, (BLOCK, ROWS), 1)

    def side_by_side(parts):
        return parts[0] if len(parts) == 1 else jnp.concatenate(parts, axis=1)

    def tile(j, slot, count, own_block=None):
        wide = count * ROWS
        rows = pl.ds(slot * ROWS, wide)
        scores = nt_dot(kbd[j], qa[rows, :])
        gp = nt_dot(vbd[j], ga[rows, :])
        for h in range(HEADS):
            off = side_by_side([offs[slot + c, j, h : h + 1, :] for c in range(count)])
            if own_block is not None:
                ok = key_at <= row_at % BLOCK
                own = jnp.where(ok, jnp.broadcast_to(meta[0, h : h + 1, :], ok.shape), NEVER)
                off = jnp.where(row_at // BLOCK == own_block, own, jnp.broadcast_to(off, ok.shape))
            dots_row = side_by_side([meta[slot + c, HEADS + h : HEADS + h + 1, :] for c in range(count)])
            part = slice(h * DH, (h + 1) * DH)
            p = jnp.exp2(scores[part] * (scale * log2e) - off)
            ps[j, part, pl.ds(slot * ROWS, wide)] = p.astype(BF16)
            ds[pl.ds(j * WIDTH + h * DH, DH), pl.ds(slot * ROWS, wide)] = (p * (gp[part] - dots_row)).astype(BF16)

    def tiles(slot, count, js):
        for j in js:
            tile(j, slot, count)

    def query_grads(slot, count):
        part = nn_dot(kbt[...], ds[:, pl.ds(slot * ROWS, count * ROWS)])
        for c in range(count):
            k = slot + c
            piece = part[:, c * ROWS : (c + 1) * ROWS]
            if k == 0:
                dq0[...] = piece
            else:
                dqs[k] = piece.astype(BF16)

    dq_sends = {k: Sends(z_of(OFFSETS[k]) > a) for k in range(1, NZ)}

    def send_query_grads(*slots, rows=None):
        def start():
            for k in slots:
                counted = dq_sends[k].size > 0
                if k == 4:
                    send(dqs.at[k], dqm, dq_sends[k], S_DM, at_z(1), counted)
                else:
                    send(dqs.at[k], dqr.at[PAIR[k]], dq_sends[k], S_DQ + PAIR[k], at_z(OFFSETS[k]), counted)

        when(rows, start)

    def key_pass_on(i):
        key_half_arrived(kx, S_K, 3, i)
        send_keys(kx, S_K, 1, i, source=3)
        key_half_arrived(vx, S_V, 1, i)
        send_keys(vx, S_V, 3, i, source=1)

    def spread_normed():
        arrived(nx.at[pl.ds(1, NX - 1)], S_N, at_x(1))
        for r in range(1, NT):
            send(nx, nt.at[t], t_sends, S_T, at_t(r))
        nt[t] = nx[...]

    def lazily(do, *args, **kwargs):
        return functools.partial(do, *args, **kwargs)

    with scope("own_tiles"):
        for i in range(2):
            tile(i, 0, 1, own_block=i)
    with scope("ring1"):
        ring_step(1, [lambda: None, lazily(key_pass_on, 0), lazily(key_pass_on, 1)], 1)
    with scope("keys_near"):
        keys_arrived(vx, S_V, 3)
        keys_arrived(kx, S_K, 1)
        lay_out_keys(1)
        lay_out_keys(3)
    with scope("ring2"):
        def last_keys():
            keys_arrived(kx, S_K, 2)
            keys_arrived(vx, S_V, 2)
            lay_out_keys(2)

        def first_grads():
            tiles(1, 2, (4, 5))
            query_grads(1, 2)
            send_query_grads(1, rows=a >= 3)

        work = [
            lazily(tiles, 0, 1, (2, 3)),
            lambda: (spread_normed(), tiles(0, 1, (6, 7))),
            lazily(tiles, 1, 2, (0, 1, 2)),
            lambda: (tiles(1, 2, (3, 6, 7)), last_keys()),
            first_grads,
        ]
        ring_step(2, work, 1)
    with scope("ring3"):
        def second_tiles(js):
            tiles(3, 2, js)

        def second_grads(js):
            tiles(3, 2, js)
            query_grads(3, 2)

        def if_early(do, *args):
            pl.when(a < 3)(functools.partial(do, *args))

        @pl.when(a >= 3)
        def _():
            second_grads(range(KB))
            send_query_grads(4, 3)

        work = [
            lambda: None,
            lazily(if_early, second_tiles, range(4)),
            lazily(send_query_grads, 1, rows=a < 3),
            lambda: (if_early(second_grads, range(4, KB)), send_query_grads(4, 3, rows=a < 3)),
        ]
        ring_step(3, work, 1)
    with scope("tiles_c"):
        tiles(5, 2, range(KB))
        query_grads(5, 2)
        send_query_grads(5, 6)

    def farthest():
        ring_step(4)
        tiles(7, 1, range(KB))

    @pl.when(a < NZ // 2)
    def _():
        with scope("farthest"):
            farthest()

    @pl.when(a >= NZ // 2)
    def _():
        cols = pl.ds(7 * ROWS, ROWS)
        ps[:, :, cols] = jnp.zeros((KB, WIDTH, ROWS), BF16)
        ds[:, cols] = jnp.zeros((KB * WIDTH, ROWS), BF16)

    with scope("farthest_dq"):
        query_grads(7, 1)
        send_query_grads(7)
    with scope("own_rest"):
        tiles(0, 1, (4, 5))
        query_grads(0, 1)

    def key_grads(r):
        for i in range(2):
            j = 2 * r + i
            gv = diagonal_heads(nn_dot(ps[j], ga[...]))
            gk = diagonal_heads(nn_dot(ds[pl.ds(j * WIDTH, WIDTH), :], qa[...])) * scale
            part = slice(i * BLOCK, (i + 1) * BLOCK)
            if r == 0:
                dv0[part, :] = gv
                dk0[part, :] = gk
            else:
                dvs[r, part, :] = gv.astype(BF16)
                dks[r, part, :] = gk.astype(BF16)

    def send_key_grads(r):
        send(dks.at[r], dkr.at[NX - r], dkv_sends, S_DK, at_x(r))
        send(dvs.at[r], dvr.at[NX - r], dkv_sends, S_DV, at_x(r))

    dkv_sends, w_sends, w2_sends = Sends(), Sends(), Sends()

    def key_grads_a():
        key_grads(2)
        key_grads(1)

    def turn_normed():
        arrived(nt.at[pl.ds(0, NT - 1)], S_T, at_t(1))
        for i, k in enumerate(TERMS):
            z = z_of(OFFSETS[k])
            for r in range(NX):
                ntt[i * FEATS : (i + 1) * FEATS, r * ROWS : (r + 1) * ROWS] = nt[z, r].T

    def side_work():
        key_grads_a()
        turn_normed()

    with scope("side_a"):
        pl.when(a >= NZ // 2)(side_work)
    with scope("dq_merge"):

        @pl.when(jnp.logical_and(a >= 1, a <= NZ - 2))
        def _():
            arrived(dqm, S_DM, at_z(-1))
            dqs[2] = (dqs[2].astype(F32) + dqm[...].astype(F32)).astype(BF16)

        send_query_grads(2)
    with scope("dq_wait"):
        for k in (1, 2, 4, 5, 6, 7):

            @pl.when(z_of(OFFSETS[k]) < a)
            def _(k=k):
                arrived(dqr.at[k], S_DQ + k, at_z(OFFSETS[k]))
                dq0[...] += dqr[k].astype(F32)

    @pl.when(a >= NZ // 2)
    def _():
        for z in range(NZ // 2):
            pl.semaphore_signal(go_sem, inc=1, device_id={"kv": z * NX + b, "tp": t}, device_id_type=MESH)

    with scope("dq_out"):
        grad_q = (dq0[...] * scale).T.astype(BF16)
        for c in range(2):
            dqx[c, 0] = grad_q[:, c * HALF : (c + 1) * HALF]
        for c in range(2):
            for r in (2, 1, 3):
                send(dqx.at[c, 0], dqx.at[c, NX - r], x_sends, S_X + c, at_x(r))
        gq_ref[...] = grad_q
    with scope("side_b"):
        pl.when(a < NZ // 2)(side_work)
        key_grads(3)
        key_grads(0)
    def gw_terms(c):
        dq_row = dqx[c].reshape(NX * ROWS, HALF)
        for first in range(0, NZ, 2):
            terms = nn_dot(ntt[first * FEATS : (first + 2) * FEATS, :], dq_row)
            for i, k in enumerate(TERMS[first : first + 2]):
                term = terms[i * FEATS : (i + 1) * FEATS]
                if k in (0, 3, 4):
                    gw_own[c, (0, 3, 4).index(k)] = term
                    continue
                gws[c, k] = term.astype(BF16)
                if k == 7:
                    send(gws.at[c, k], gw4.at[c], w_sends, S_W4 + c, at_z(4 * c - 2))
                elif k in (5, 6):
                    send(gws.at[c, k], gw3.at[c, k - 5], w_sends, S_W3[c] + k - 5, at_z(-1 if k == 5 else 1))
                else:
                    send(gws.at[c, k], gwr.at[c, PAIR[k]], w_sends, S_W, at_z(OFFSETS[k]))

    def gw_pass_on(c):
        for side in (1 - c, c):
            k = 3 + side
            arrived(gw3.at[c, side], S_W3[c] + side, at_z(1 - 2 * side))
            term = gw_own[c, 1 + side] + gw3[c, side].astype(F32)
            if side == c:
                arrived(gw4.at[c], S_W4 + c, at_z(2 - 4 * c))
                term = term + gw4[c].astype(F32)
            gws[c, k] = term.astype(BF16)
            send(gws.at[c, k], gwr.at[c, PAIR[k]], w2_sends, S_W, at_z(OFFSETS[k]))

    with scope("go"):

        @pl.when(a < NZ // 2)
        def _():
            pl.semaphore_wait(go_sem, NZ // 2)

    for c in range(2):
        with scope(f"dqx{c}"):
            arrived(dqx.at[c, pl.ds(1, NX - 1)], S_X + c, at_x(1))
        with scope(f"gw{c}"):
            gw_terms(c)
    for r in (2, 1, 3):
        send_key_grads(r)
    for c in range(2):
        with scope(f"gw_pass_on{c}"):
            gw_pass_on(c)

    with scope("dkv_wait"):
        arrived(dkr.at[pl.ds(1, NX - 1)], S_DK, at_x(1))
        arrived(dvr.at[pl.ds(1, NX - 1)], S_DV, at_x(1))
        sum_k, sum_v = dk0[...], dv0[...]
        for r in range(1, NX):
            sum_k = sum_k + dkr[r].astype(F32)
            sum_v = sum_v + dvr[r].astype(F32)
        gk_ref[...] = sum_k.astype(BF16)
        gv_ref[...] = sum_v.astype(BF16)

    with scope("gw_wait"):
        arrived(qa.at[pl.ds(0, 4 * ROWS), :], S_W, at_z(1))
        for c in range(2):
            total_w = gw_own[c, 0]
            for k in range(1, 5):
                total_w = total_w + gwr[c, k].astype(F32)
            gw_ref[:, c * HALF : (c + 1) * HALF] = total_w
    with scope("end"):
        for group in groups:
            group.finish()
        assert counts == [SENDS, ARRIVALS], counts


def put_out(*refs):
    stores = [pltpu.make_async_copy(refs[i], refs[4 + i], refs[8].at[i]) for i in range(4)]
    for copy in stores:
        copy.start()
    for copy in stores:
        copy.wait()


def local(queries, keys, values, attended, cotangent, log_totals, block_picks, normed):
    vmem = pl.BlockSpec(memory_space=pltpu.VMEM)
    hbm = pl.BlockSpec(memory_space=pltpu.HBM)
    b16 = lambda *shape: pltpu.VMEM(shape, BF16)
    f32 = lambda *shape: pltpu.VMEM(shape, F32)
    shapes = (
        jax.ShapeDtypeStruct((ROWS, WIDTH), BF16),
        jax.ShapeDtypeStruct((ROWS, WIDTH), BF16),
        jax.ShapeDtypeStruct((ROWS, WIDTH), BF16),
        jax.ShapeDtypeStruct((FEATS, WIDTH), F32),
    )
    grads = pl.pallas_call(
        kernel,
        out_shape=tuple(pltpu.VMEM(x.shape, x.dtype) for x in shapes),
        in_specs=[hbm] * 8,
        out_specs=(vmem,) * 4,
        scratch_shapes=[
            b16(ROWS, WIDTH), f32(HEADS, ROWS), pltpu.VMEM((HEADS, 2, SEL), jnp.int32), b16(ROWS, NX * FEATS),
            b16(NZ * ROWS, WIDTH), b16(NZ * ROWS, WIDTH), f32(NZ, 16, ROWS), f32(NZ, KB, 8, ROWS),
            b16(NX, ROWS, WIDTH), b16(NX, ROWS, WIDTH),
            b16(KB, WIDTH, WIDTH), b16(KB, WIDTH, WIDTH), b16(WIDTH, KB * WIDTH),
            b16(KB, WIDTH, NZ * ROWS), b16(KB * WIDTH, NZ * ROWS),
            b16(NZ, WIDTH, ROWS), b16(NZ, WIDTH, ROWS), b16(WIDTH, ROWS), f32(WIDTH, ROWS),
            b16(NX, ROWS, FEATS), b16(NT, NX, ROWS, FEATS), b16(NZ * FEATS, NX * ROWS),
            b16(2, NX, ROWS, HALF),
            b16(NX, ROWS, WIDTH), b16(NX, ROWS, WIDTH), b16(NX, ROWS, WIDTH), b16(NX, ROWS, WIDTH),
            f32(ROWS, WIDTH), f32(ROWS, WIDTH),
            b16(2, NZ, FEATS, HALF), b16(2, 5, FEATS, HALF),
            b16(2, 2, FEATS, HALF), b16(2, FEATS, HALF), f32(2, 3, FEATS, HALF),
            pltpu.SemaphoreType.DMA((9,)),
            pltpu.SemaphoreType.DMA((SENDS,)),
            pltpu.SemaphoreType.DMA((ARRIVALS,)),
            pltpu.SemaphoreType.REGULAR,
        ],
        compiler_params=pltpu.CompilerParams(
            collective_id=0, has_side_effects=True, vmem_limit_bytes=MAIN_VMEM
        ),
        name="attention_grads",
    )(queries, keys, values, attended, cotangent, log_totals, block_picks, normed)
    return pl.pallas_call(
        put_out,
        out_shape=shapes,
        in_specs=[vmem] * 4,
        out_specs=(hbm,) * 4,
        scratch_shapes=[pltpu.SemaphoreType.DMA((4,))],
        compiler_params=pltpu.CompilerParams(vmem_limit_bytes=1024 * 1024),
        name="put_out",
    )(*grads)


def solution(mesh):
    in_specs = (
        P("kv", "tp"),
        P("kv", "tp"),
        P("kv", "tp"),
        P("kv", "tp"),
        P("kv", "tp"),
        P("tp", "kv"),
        P("tp", "kv", None),
        P("kv", "tp"),
    )
    out_specs = (P("kv", "tp"), P("kv", "tp"), P("kv", "tp"), P("kv", "tp"))
    return jax.shard_map(local, mesh=mesh, in_specs=in_specs, out_specs=out_specs, check_vma=False)
```

```python
import functools
import math

import jax
import jax.numpy as jnp
from jax import lax
from jax.experimental import pallas as pl
from jax.experimental.pallas import tpu as pltpu
from jax.sharding import PartitionSpec as P

MESH = pl.DeviceIdType.MESH
BLOCK = 64
NZ, NX, NT = 8, 4, 8
ROWS = 128
WIDTH = 256
HEADS, DH = 4, 64
SEL = 8
FEATS = 128
KB = 2 * NX
NEVER = 1e30
MAIN_VMEM = 67043328 - (3 * 64 + 128) * 1024
SENDS, ARRIVALS = 28, 64
HALF = WIDTH // 2
F32, BF16 = jnp.float32, jnp.bfloat16

UP, DOWN = NZ // 2, NZ // 2 - 1


def up_slot(s):
    return 2 * s - 1


def down_slot(s):
    return 2 * s if s < NZ // 2 else NZ - 1


OFFSETS = [0] + [None] * (NZ - 1)
for _s in range(1, NZ // 2 + 1):
    OFFSETS[up_slot(_s)] = -_s
for _s in range(1, NZ // 2):
    OFFSETS[down_slot(_s)] = _s
PAIR = [0] + [OFFSETS.index(-o) if -o in OFFSETS else NZ - 1 for o in OFFSETS[1:]]
TERMS = (7, 6, 5, 2, 1, 3, 4, 0)


def nt_dot(a, b):
    return lax.dot_general(a, b, (((1,), (1,)), ((), ())), preferred_element_type=F32)


def nn_dot(a, b):
    return lax.dot_general(a, b, (((1,), (0,)), ((), ())), preferred_element_type=F32)


def diagonal_heads(m):
    lane_head = lax.broadcasted_iota(jnp.int32, (DH, WIDTH), 1) // DH
    out = m[(HEADS - 1) * DH :]
    for h in range(HEADS - 1):
        out = jnp.where(lane_head == h, m[h * DH : (h + 1) * DH], out)
    return out


def kernel(
    q_hbm, k_hbm, v_hbm, o_hbm, g_hbm, l_hbm, pick_hbm, n_hbm,
    gq_ref, gk_ref, gv_ref, gw_ref,
    o_ref, l_ref, pick_ref, n_ref,
    qa, ga, meta, offs, kx, vx, kbd, vbd, kbt, ps, ds, dqs, dqr, dqm, dq0,
    nx, nt, ntt, dqx, dks, dvs, dkr, dvr, dk0, dv0, gws, gwr, gw3, gw4, gw_own,
    load_sem, send_sem, recv_sem, go_sem,
):
    kv = lax.axis_index("kv")
    t = lax.axis_index("tp")
    a = kv // NX
    b = kv % NX
    scale = DH**-0.5
    log2e = 1.0 / math.log(2.0)
    scope = jax.named_scope

    def z_of(off):
        return (a + NZ + off) % NZ

    def at_z(off):
        return {"kv": z_of(off) * NX + b, "tp": t}

    def at_x(r):
        return {"kv": a * NX + (b + r) % NX, "tp": t}

    def at_t(r):
        return {"kv": kv, "tp": (t + r) % NT}

    counts = [0, 0]

    def take(which, n):
        first = counts[which]
        counts[which] += n
        return first

    def arrivals(n=1):
        return take(1, n)

    class Sends:
        def __init__(self, cond=None):
            self.at, self.cond, self.size = take(0, 1), cond, 0
            groups.append(self)

        def finish(self):
            like = qa if self.size <= 2 * NZ * ROWS * WIDTH else ds
            ref = like.at[pl.ds(0, self.size // (2 * like.shape[1])), :]
            copy = pltpu.make_async_remote_copy(
                src_ref=ref, dst_ref=ref, send_sem=send_sem.at[self.at], recv_sem=recv_sem.at[0],
                device_id=at_x(1), device_id_type=MESH,
            )
            when(self.cond, copy.wait_send)

    groups = []

    S_RING = [arrivals(NZ - 1) - 1 for _ in range(5)]
    S_K = [(arrivals(), arrivals()) if r == 3 else (arrivals(),) * 2 for r in range(1, NX)]
    S_V = [(arrivals(), arrivals()) if r == 1 else (arrivals(),) * 2 for r in range(1, NX)]
    S_N, S_T, S_DQ, S_DK, S_DV, S_X = arrivals(), arrivals(), arrivals(NZ - 1) - 1, arrivals(), arrivals(), arrivals(2)
    S_DM = arrivals()
    S_W3, S_W4, S_W = (arrivals(2), arrivals(2)), arrivals(2), arrivals()

    def when(cond, do):
        if cond is None:
            do()
        else:
            pl.when(cond)(do)

    def send(src, dst, group, at_theirs, dev, counted=False):
        copy = pltpu.make_async_remote_copy(
            src_ref=src, dst_ref=dst, send_sem=send_sem.at[group.at], recv_sem=recv_sem.at[at_theirs],
            device_id=dev, device_id_type=MESH,
        )
        when(group.cond, copy.start)
        group.size += 0 if counted else math.prod(src.shape) * jnp.dtype(src.dtype).itemsize

    def arrived(dst, at_mine, dev):
        pltpu.make_async_remote_copy(
            src_ref=dst, dst_ref=dst, send_sem=send_sem.at[0], recv_sem=recv_sem.at[at_mine],
            device_id=dev, device_id_type=MESH,
        ).wait_recv()

    def slot_rows(slot):
        return pl.ds(slot * ROWS, ROWS)

    def half(ref, slot, i):
        return ref.at[pl.ds(slot * ROWS + i * BLOCK, BLOCK), :]

    own_cols = pl.ds(pl.multiple_of(b * FEATS, FEATS), FEATS)
    loads = [
        pltpu.make_async_copy(src, dst, load_sem.at[i])
        for i, (src, dst) in enumerate((
            (q_hbm, qa.at[slot_rows(0), :]), (g_hbm, ga.at[slot_rows(0), :]), (k_hbm, kx.at[0]), (v_hbm, vx.at[0]),
            (o_hbm, o_ref), (l_hbm, l_ref), (pick_hbm, pick_ref), (n_hbm, n_ref), (n_hbm.at[:, own_cols], nx.at[0]),
        ))
    ]
    for copy in loads:
        copy.start()

    barrier = pltpu.get_barrier_semaphore()
    peers = [at_t(r) for r in range(1, NT)] + [at_x(r) for r in range(1, NX)] + [at_z(1), at_z(-1)]
    for dev in peers:
        pl.semaphore_signal(barrier, inc=1, device_id=dev, device_id_type=MESH)
    with scope("load"):
        for copy in loads:
            copy.wait()

    prod = ga[slot_rows(0), :].astype(F32) * o_ref[...].astype(F32)
    high = prod.astype(BF16)
    low = (prod - high.astype(F32)).astype(BF16)
    ones = (
        lax.broadcasted_iota(jnp.int32, (8, WIDTH), 1) // DH == lax.broadcasted_iota(jnp.int32, (8, WIDTH), 0)
    ).astype(BF16)
    dots = nt_dot(ones, high) + nt_dot(ones, low)
    meta[0, 0:HEADS, :] = l_ref[...] * log2e
    meta[0, HEADS : 2 * HEADS, :] = dots[0:HEADS]
    meta[0, 8:16, :] = jnp.full((8, ROWS), -2.0, F32)
    for h in range(HEADS):
        for c in range(2):
            meta[0, 8 + c * HEADS + h : 9 + c * HEADS + h, 0:SEL] = pick_ref[h, c : c + 1, :].astype(F32)

    first_block = lax.broadcasted_iota(jnp.int32, (HEADS, ROWS), 1) < BLOCK

    def offsets(slot):
        for j in range(KB):
            block_id = (a * KB + 2 * ((b + j // 2) % NX) + j % 2).astype(F32)
            hit = jnp.where(meta[slot, 8:16, :] == block_id, 1.0, 0.0)
            hit = jnp.max(hit, axis=1, keepdims=True)
            named = jnp.where(first_block, hit[0:HEADS], hit[HEADS : 2 * HEADS]) > 0.5
            offs[slot, j, 0:HEADS, :] = jnp.where(named, meta[slot, 0:HEADS, :], NEVER)

    with scope("barrier"):
        pl.semaphore_wait(barrier, len(peers))

    up_order = [("m", UP), ("q0", UP), ("q1", UP), ("g0", DOWN), ("g1", DOWN)]
    down_order = [("g0", UP), ("g1", UP), ("m", DOWN), ("q0", DOWN), ("q1", DOWN)]
    names = ["m", "q0", "q1", "g0", "g1"]

    def piece_at(name, slot):
        if name == "m":
            return meta.at[slot]
        return half(qa if name[0] == "q" else ga, slot, int(name[1]))

    def flows(down, limit, s):
        return a + s < NZ if down else z_of(-s) >= NZ - limit

    def flows_on(down, limit, s):
        return jnp.logical_and(a + s < NZ, a >= 1) if down else z_of(-s) >= NZ - limit

    def clear(ref):
        ref[...] = jnp.zeros(ref.shape, ref.dtype)

    def ring_step(s, between=(), each=2):
        between = list(between)
        sends = {
            (down, limit): Sends(flows_on(down, limit, s)) for down in (False, True) for limit in (UP, DOWN) if s < limit
        }
        for pieces in zip(up_order, down_order):
            for (name, limit), down in zip(pieces, (False, True)):
                sem = S_RING[names.index(name)]
                slot_of, to = (down_slot, -1) if down else (up_slot, 1)
                if 0 < s <= limit:
                    piece, at, comes = piece_at(name, slot_of(s)), sem + slot_of(s), flows(down, limit, s)
                    pl.when(comes)(functools.partial(arrived, piece, at, at_z(-to)))
                    pl.when(jnp.logical_not(comes))(functools.partial(clear, piece))
                    if name == "m":
                        offsets(slot_of(s))
                if s < limit:
                    there = slot_of(s + 1)
                    src = piece_at(name, slot_of(s) if s else 0)
                    send(src, piece_at(name, there), sends[down, limit], sem + there, at_z(to))
            for do in between[:each]:
                do()
            between = between[each:]
        for do in between:
            do()

    def key_half(ref, r, i):
        return ref.at[r, pl.ds(i * BLOCK, BLOCK), :]

    def send_keys(ref, first, r, i, source=0):
        there = (source - r) % NX
        send(key_half(ref, source, i), key_half(ref, there, i), key_sends, first[there - 1][i], at_x(r))

    def key_half_arrived(ref, first, r, i):
        arrived(key_half(ref, r, i), first[r - 1][i], at_x(r))

    def keys_arrived(ref, first, r):
        arrived(ref.at[r], first[r - 1][0], at_x(r))

    key_sends, n_sends, t_sends, x_sends = Sends(), Sends(), Sends(), Sends()
    with scope("start"):
        ring_step(0)
        for i in range(2):
            send_keys(kx, S_K, 1, i)
            send_keys(vx, S_V, 3, i)
        for i in range(2):
            send_keys(vx, S_V, 1, i)
            send_keys(kx, S_K, 3, i)
        for r in (1, 3, 2):
            there = (b + r) % NX
            cols = pl.ds(pl.multiple_of(there * FEATS, FEATS), FEATS)
            send(n_ref.at[:, cols], nx.at[NX - r], n_sends, S_N, at_x(r))

    lane_head = lax.broadcasted_iota(jnp.int32, (BLOCK, WIDTH), 1) // DH
    t_head = lax.broadcasted_iota(jnp.int32, (WIDTH, 2 * BLOCK), 0) // DH
    t_half = lax.broadcasted_iota(jnp.int32, (WIDTH, 2 * BLOCK), 1) // BLOCK

    def lay_out_keys(r):
        for i in range(2):
            j = 2 * r + i
            kb = kx[r, i * BLOCK : (i + 1) * BLOCK, :]
            vb = vx[r, i * BLOCK : (i + 1) * BLOCK, :]
            zero = jnp.zeros_like(kb)
            for h in range(HEADS):
                kbd[j, h * DH : (h + 1) * DH, :] = jnp.where(lane_head == h, kb, zero)
                vbd[j, h * DH : (h + 1) * DH, :] = jnp.where(lane_head == h, vb, zero)
            turned = jnp.concatenate([kb, kb], axis=0).T
            for hh in range(HEADS // 2):
                kbt[:, pl.ds(j * WIDTH + hh * ROWS, ROWS)] = jnp.where(
                    t_head == 2 * hh + t_half, turned, jnp.zeros_like(turned)
                )

    with scope("lay0"):
        lay_out_keys(0)
        offsets(0)

    key_at = lax.broadcasted_iota(jnp.int32, (BLOCK, ROWS), 0)
    row_at = lax.broadcasted_iota(jnp.int32, (BLOCK, ROWS), 1)

    def side_by_side(parts):
        return parts[0] if len(parts) == 1 else jnp.concatenate(parts, axis=1)

    def tile(j, slot, count, own_block=None):
        wide = count * ROWS
        rows = pl.ds(slot * ROWS, wide)
        scores = nt_dot(kbd[j], qa[rows, :])
        gp = nt_dot(vbd[j], ga[rows, :])
        for h in range(HEADS):
            off = side_by_side([offs[slot + c, j, h : h + 1, :] for c in range(count)])
            if own_block is not None:
                ok = key_at <= row_at % BLOCK
                own = jnp.where(ok, jnp.broadcast_to(meta[0, h : h + 1, :], ok.shape), NEVER)
                off = jnp.where(row_at // BLOCK == own_block, own, jnp.broadcast_to(off, ok.shape))
            dots_row = side_by_side([meta[slot + c, HEADS + h : HEADS + h + 1, :] for c in range(count)])
            part = slice(h * DH, (h + 1) * DH)
            p = jnp.exp2(scores[part] * (scale * log2e) - off)
            ps[j, part, pl.ds(slot * ROWS, wide)] = p.astype(BF16)
            ds[pl.ds(j * WIDTH + h * DH, DH), pl.ds(slot * ROWS, wide)] = (p * (gp[part] - dots_row)).astype(BF16)

    def tiles(slot, count, js):
        for j in js:
            tile(j, slot, count)

    def query_grads(slot, count):
        part = nn_dot(kbt[...], ds[:, pl.ds(slot * ROWS, count * ROWS)])
        for c in range(count):
            k = slot + c
            piece = part[:, c * ROWS : (c + 1) * ROWS]
            if k == 0:
                dq0[...] = piece
            else:
                dqs[k] = piece.astype(BF16)

    dq_sends = {k: Sends(z_of(OFFSETS[k]) > a) for k in range(1, NZ)}

    def send_query_grads(*slots, rows=None):
        def start():
            for k in slots:
                counted = dq_sends[k].size > 0
                if k == 4:
                    send(dqs.at[k], dqm, dq_sends[k], S_DM, at_z(1), counted)
                else:
                    send(dqs.at[k], dqr.at[PAIR[k]], dq_sends[k], S_DQ + PAIR[k], at_z(OFFSETS[k]), counted)

        when(rows, start)

    def key_pass_on(i):
        key_half_arrived(kx, S_K, 3, i)
        send_keys(kx, S_K, 1, i, source=3)
        key_half_arrived(vx, S_V, 1, i)
        send_keys(vx, S_V, 3, i, source=1)

    def spread_normed():
        arrived(nx.at[pl.ds(1, NX - 1)], S_N, at_x(1))
        for r in range(1, NT):
            send(nx, nt.at[t], t_sends, S_T, at_t(r))
        nt[t] = nx[...]

    def lazily(do, *args, **kwargs):
        return functools.partial(do, *args, **kwargs)

    with scope("own_tiles"):
        for i in range(2):
            tile(i, 0, 1, own_block=i)
    with scope("ring1"):
        ring_step(1, [lambda: None, lazily(key_pass_on, 0), lazily(key_pass_on, 1)], 1)
    with scope("keys_near"):
        keys_arrived(vx, S_V, 3)
        keys_arrived(kx, S_K, 1)
        lay_out_keys(1)
        lay_out_keys(3)
    with scope("ring2"):
        def last_keys():
            keys_arrived(kx, S_K, 2)
            keys_arrived(vx, S_V, 2)
            lay_out_keys(2)

        def first_grads():
            tiles(1, 2, (4, 5))
            query_grads(1, 2)
            send_query_grads(1, rows=a >= 3)

        work = [
            lazily(tiles, 0, 1, (2, 3)),
            lambda: (spread_normed(), tiles(0, 1, (6, 7))),
            lazily(tiles, 1, 2, (0, 1, 2)),
            lambda: (tiles(1, 2, (3, 6, 7)), last_keys()),
            first_grads,
        ]
        ring_step(2, work, 1)
    with scope("ring3"):
        def second_tiles(js):
            tiles(3, 2, js)

        def second_grads(js):
            tiles(3, 2, js)
            query_grads(3, 2)

        def if_early(do, *args):
            pl.when(a < 3)(functools.partial(do, *args))

        @pl.when(a >= 3)
        def _():
            second_grads(range(KB))
            send_query_grads(4, 3)

        work = [
            lambda: None,
            lazily(if_early, second_tiles, range(4)),
            lazily(send_query_grads, 1, rows=a < 3),
            lambda: (if_early(second_grads, range(4, KB)), send_query_grads(4, 3, rows=a < 3)),
        ]
        ring_step(3, work, 1)
    with scope("tiles_c"):
        tiles(5, 2, range(KB))
        query_grads(5, 2)
        send_query_grads(5, 6)

    def farthest():
        ring_step(4)
        tiles(7, 1, range(KB))

    @pl.when(a < NZ // 2)
    def _():
        with scope("farthest"):
            farthest()

    @pl.when(a >= NZ // 2)
    def _():
        cols = pl.ds(7 * ROWS, ROWS)
        ps[:, :, cols] = jnp.zeros((KB, WIDTH, ROWS), BF16)
        ds[:, cols] = jnp.zeros((KB * WIDTH, ROWS), BF16)

    with scope("farthest_dq"):
        query_grads(7, 1)
        send_query_grads(7)
    with scope("own_rest"):
        tiles(0, 1, (4, 5))
        query_grads(0, 1)

    def key_grads(r):
        for i in range(2):
            j = 2 * r + i
            gv = diagonal_heads(nn_dot(ps[j], ga[...]))
            gk = diagonal_heads(nn_dot(ds[pl.ds(j * WIDTH, WIDTH), :], qa[...])) * scale
            part = slice(i * BLOCK, (i + 1) * BLOCK)
            if r == 0:
                dv0[part, :] = gv
                dk0[part, :] = gk
            else:
                dvs[r, part, :] = gv.astype(BF16)
                dks[r, part, :] = gk.astype(BF16)

    def send_key_grads(r):
        send(dks.at[r], dkr.at[NX - r], dkv_sends, S_DK, at_x(r))
        send(dvs.at[r], dvr.at[NX - r], dkv_sends, S_DV, at_x(r))

    dkv_sends, w_sends, w2_sends = Sends(), Sends(), Sends()

    def key_grads_a():
        key_grads(2)
        key_grads(1)

    def turn_normed():
        arrived(nt.at[pl.ds(0, NT - 1)], S_T, at_t(1))
        for i, k in enumerate(TERMS):
            z = z_of(OFFSETS[k])
            for r in range(NX):
                ntt[i * FEATS : (i + 1) * FEATS, r * ROWS : (r + 1) * ROWS] = nt[z, r].T

    def side_work():
        key_grads_a()
        turn_normed()

    with scope("side_a"):
        pl.when(a >= NZ // 2)(side_work)
    with scope("dq_merge"):

        @pl.when(jnp.logical_and(a >= 1, a <= NZ - 2))
        def _():
            arrived(dqm, S_DM, at_z(-1))
            dqs[2] = (dqs[2].astype(F32) + dqm[...].astype(F32)).astype(BF16)

        send_query_grads(2)
    with scope("dq_wait"):
        for k in (1, 2, 4, 5, 6, 7):

            @pl.when(z_of(OFFSETS[k]) < a)
            def _(k=k):
                arrived(dqr.at[k], S_DQ + k, at_z(OFFSETS[k]))
                dq0[...] += dqr[k].astype(F32)

    @pl.when(a >= NZ // 2)
    def _():
        for z in range(NZ // 2):
            pl.semaphore_signal(go_sem, inc=1, device_id={"kv": z * NX + b, "tp": t}, device_id_type=MESH)

    with scope("dq_out"):
        grad_q = (dq0[...] * scale).T.astype(BF16)
        for c in range(2):
            dqx[c, 0] = grad_q[:, c * HALF : (c + 1) * HALF]
        for c in range(2):
            for r in (2, 1, 3):
                send(dqx.at[c, 0], dqx.at[c, NX - r], x_sends, S_X + c, at_x(r))
        gq_ref[...] = grad_q
    with scope("side_b"):
        pl.when(a < NZ // 2)(side_work)
        key_grads(3)
        key_grads(0)
    def gw_terms(c):
        dq_row = dqx[c].reshape(NX * ROWS, HALF)
        for first in range(0, NZ, 2):
            terms = nn_dot(ntt[first * FEATS : (first + 2) * FEATS, :], dq_row)
            for i, k in enumerate(TERMS[first : first + 2]):
                term = terms[i * FEATS : (i + 1) * FEATS]
                if k in (0, 3, 4):
                    gw_own[c, (0, 3, 4).index(k)] = term
                    continue
                gws[c, k] = term.astype(BF16)
                if k == 7:
                    send(gws.at[c, k], gw4.at[c], w_sends, S_W4 + c, at_z(4 * c - 2))
                elif k in (5, 6):
                    send(gws.at[c, k], gw3.at[c, k - 5], w_sends, S_W3[c] + k - 5, at_z(-1 if k == 5 else 1))

    def send_near_terms(c):
        for k in (1, 2):
            send(gws.at[c, k], gwr.at[c, PAIR[k]], w_sends, S_W, at_z(OFFSETS[k]))

    def gw_pass_on(c):
        for side in (1 - c, c):
            k = 3 + side
            arrived(gw3.at[c, side], S_W3[c] + side, at_z(1 - 2 * side))
            term = gw_own[c, 1 + side] + gw3[c, side].astype(F32)
            if side == c:
                arrived(gw4.at[c], S_W4 + c, at_z(2 - 4 * c))
                term = term + gw4[c].astype(F32)
            gws[c, k] = term.astype(BF16)
            send(gws.at[c, k], gwr.at[c, PAIR[k]], w2_sends, S_W, at_z(OFFSETS[k]))

    with scope("go"):

        @pl.when(a < NZ // 2)
        def _():
            pl.semaphore_wait(go_sem, NZ // 2)

    for c in range(2):
        with scope(f"dqx{c}"):
            arrived(dqx.at[c, pl.ds(1, NX - 1)], S_X + c, at_x(1))
        with scope(f"gw{c}"):
            gw_terms(c)
    for c in range(2):
        send_near_terms(c)
    for r in (2, 1, 3):
        send_key_grads(r)
    for c in range(2):
        with scope(f"gw_pass_on{c}"):
            gw_pass_on(c)

    with scope("dkv_wait"):
        arrived(dkr.at[pl.ds(1, NX - 1)], S_DK, at_x(1))
        arrived(dvr.at[pl.ds(1, NX - 1)], S_DV, at_x(1))
        sum_k, sum_v = dk0[...], dv0[...]
        for r in range(1, NX):
            sum_k = sum_k + dkr[r].astype(F32)
            sum_v = sum_v + dvr[r].astype(F32)
        gk_ref[...] = sum_k.astype(BF16)
        gv_ref[...] = sum_v.astype(BF16)

    with scope("gw_wait"):
        arrived(qa.at[pl.ds(0, 4 * ROWS), :], S_W, at_z(1))
        for c in range(2):
            total_w = gw_own[c, 0]
            for k in range(1, 5):
                total_w = total_w + gwr[c, k].astype(F32)
            gw_ref[:, c * HALF : (c + 1) * HALF] = total_w
    with scope("end"):
        for group in groups:
            group.finish()
        assert counts == [SENDS, ARRIVALS], counts


def put_out(*refs):
    stores = [pltpu.make_async_copy(refs[i], refs[4 + i], refs[8].at[i]) for i in range(4)]
    for copy in stores:
        copy.start()
    for copy in stores:
        copy.wait()


def local(queries, keys, values, attended, cotangent, log_totals, block_picks, normed):
    vmem = pl.BlockSpec(memory_space=pltpu.VMEM)
    hbm = pl.BlockSpec(memory_space=pltpu.HBM)
    b16 = lambda *shape: pltpu.VMEM(shape, BF16)
    f32 = lambda *shape: pltpu.VMEM(shape, F32)
    shapes = (
        jax.ShapeDtypeStruct((ROWS, WIDTH), BF16),
        jax.ShapeDtypeStruct((ROWS, WIDTH), BF16),
        jax.ShapeDtypeStruct((ROWS, WIDTH), BF16),
        jax.ShapeDtypeStruct((FEATS, WIDTH), F32),
    )
    grads = pl.pallas_call(
        kernel,
        out_shape=tuple(pltpu.VMEM(x.shape, x.dtype) for x in shapes),
        in_specs=[hbm] * 8,
        out_specs=(vmem,) * 4,
        scratch_shapes=[
            b16(ROWS, WIDTH), f32(HEADS, ROWS), pltpu.VMEM((HEADS, 2, SEL), jnp.int32), b16(ROWS, NX * FEATS),
            b16(NZ * ROWS, WIDTH), b16(NZ * ROWS, WIDTH), f32(NZ, 16, ROWS), f32(NZ, KB, 8, ROWS),
            b16(NX, ROWS, WIDTH), b16(NX, ROWS, WIDTH),
            b16(KB, WIDTH, WIDTH), b16(KB, WIDTH, WIDTH), b16(WIDTH, KB * WIDTH),
            b16(KB, WIDTH, NZ * ROWS), b16(KB * WIDTH, NZ * ROWS),
            b16(NZ, WIDTH, ROWS), b16(NZ, WIDTH, ROWS), b16(WIDTH, ROWS), f32(WIDTH, ROWS),
            b16(NX, ROWS, FEATS), b16(NT, NX, ROWS, FEATS), b16(NZ * FEATS, NX * ROWS),
            b16(2, NX, ROWS, HALF),
            b16(NX, ROWS, WIDTH), b16(NX, ROWS, WIDTH), b16(NX, ROWS, WIDTH), b16(NX, ROWS, WIDTH),
            f32(ROWS, WIDTH), f32(ROWS, WIDTH),
            b16(2, NZ, FEATS, HALF), b16(2, 5, FEATS, HALF),
            b16(2, 2, FEATS, HALF), b16(2, FEATS, HALF), f32(2, 3, FEATS, HALF),
            pltpu.SemaphoreType.DMA((9,)),
            pltpu.SemaphoreType.DMA((SENDS,)),
            pltpu.SemaphoreType.DMA((ARRIVALS,)),
            pltpu.SemaphoreType.REGULAR,
        ],
        compiler_params=pltpu.CompilerParams(
            collective_id=0, has_side_effects=True, vmem_limit_bytes=MAIN_VMEM
        ),
        name="attention_grads",
    )(queries, keys, values, attended, cotangent, log_totals, block_picks, normed)
    return pl.pallas_call(
        put_out,
        out_shape=shapes,
        in_specs=[vmem] * 4,
        out_specs=(hbm,) * 4,
        scratch_shapes=[pltpu.SemaphoreType.DMA((4,))],
        compiler_params=pltpu.CompilerParams(vmem_limit_bytes=1024 * 1024),
        name="put_out",
    )(*grads)


def solution(mesh):
    in_specs = (
        P("kv", "tp"),
        P("kv", "tp"),
        P("kv", "tp"),
        P("kv", "tp"),
        P("kv", "tp"),
        P("tp", "kv"),
        P("tp", "kv", None),
        P("kv", "tp"),
    )
    out_specs = (P("kv", "tp"), P("kv", "tp"), P("kv", "tp"), P("kv", "tp"))
    return jax.shard_map(local, mesh=mesh, in_specs=in_specs, out_specs=out_specs, check_vma=False)
```
